128 devices in a mesh: sp: 64 (over z, y, x), tp: 2 (over core).
Axes of the slice: x: 4, y: 4, z: 4, core: 2. Of those that a mesh axis runs over, the one named last changes fastest.
Arguments:
- stream: bfloat16 [16384, 2048], P('sp', 'tp'), may hold values from -80 to 80
- norm_gain: float32 [2048], P('tp'), may hold values from 0.1 to 1.9
- cotangent: bfloat16 [16384, 2048], P('sp', 'tp'), may hold values from -16 to 16
- route_weights: float32 [16384, 2], P('sp'), may hold values from 0.1 to 1.5
- routes: int32 [16384, 2], P('sp'), may hold values from 0 to 63, all different within a row; in each aligned block of 256 rows (0 to 255, 256 to 511, ...) at most 16 rows name the same one
- conv_input: bfloat16 [16384, 1024], P('sp', 'tp'), may hold values from -6 to 6
- conv_bgate: bfloat16 [16384, 1024], P('sp', 'tp'), may hold values from -6 to 6
- conv_cgate: bfloat16 [16384, 1024], P('sp', 'tp'), may hold values from -6 to 6
- conv_taps: float32 [3, 1024], P(None, 'tp'), may hold values from -3 to 3
- out_proj: bfloat16 [2048, 1024], P(None, 'tp'), may hold values from -0.1875 to 0.1875
- gate_weight: bfloat16 [64, 2048, 1024], P('sp', None, 'tp'), may hold values from -0.125 to 0.125
- up_weight: bfloat16 [64, 2048, 1024], P('sp', None, 'tp'), may hold values from -0.125 to 0.125
- down_weight: bfloat16 [64, 1024, 2048], P('sp', 'tp'), may hold values from -0.1875 to 0.1875
Outputs:
- stream_grad: bfloat16 [16384, 2048], P('sp', 'tp')
- proj_grad: float32 [2048, 1024], P('sp', 'tp')
- input_grad: bfloat16 [16384, 1024], P('sp', 'tp')
- bgate_grad: bfloat16 [16384, 1024], P('sp', 'tp')
- cgate_grad: bfloat16 [16384, 1024], P('sp', 'tp')
- gate_grad: float32 [64, 2048, 1024], P('sp', None, 'tp')
- up_grad: float32 [64, 2048, 1024], P('sp', None, 'tp')
- down_grad: float32 [64, 1024, 2048], P('sp', 'tp')
The draws below stay inside these ranges and needn't reach their ends.
Inputs may be any that keep to these rules, and one draw needn't show every extreme that they name: `routes`: the 2 experts of a token differ. Among the tokens of one index of sp, no expert is named more than 16 times, a bound that some block reaches.
All inputs are finite; a program needn't handle non-finite values.
Results may differ from the reference program's by a relative error of at most 0.003.
The reference program's roundings to bfloat16 on the way count: a program that leaves them out, or rounds other values in their place, can miss the bound.
Values may be sent and summed in bfloat16 or wider, within the bound.
No kernel may reach another device: no remote copies, remote signals or barrier semaphores. Data moves between devices by JAX's collectives and lax.ppermute only.
A program may use at most 128 MiB of HBM per device.

```python
import math
import jax
import jax.numpy as jnp
import numpy as np
from jax import lax

D = 2048
CW = 1024
EH = 1024
K = 2
TOK_DEV = 256
TOKENS = 16384
EXPERTS = 64
CAP = 16
N_SP = 64
N_TP = 2


def draw_stream(key, part):
    keys = jax.random.split(key, 3)
    row_scale = jnp.exp(jax.random.uniform(keys[0], (TOKENS, 1), jnp.float32, 0.0, 2.3))
    column_rise = 3.0 ** (jnp.arange(D, dtype=jnp.float32) / D)
    column_scale = column_rise[None, :] * jnp.exp(jax.random.uniform(keys[1], (1, D), jnp.float32, -0.5, 0.5))
    values = jax.random.normal(keys[2], (TOKENS, D), jnp.float32)
    return jnp.clip(values * row_scale * column_scale, -80.0, 80.0).astype(jnp.bfloat16)


def spiked(array, key, source, target, parts, factor):
    def block_of(axis_at):
        return (jnp.arange(array.shape[axis_at]) // (array.shape[axis_at] // parts)).reshape((-1,) + (1,) * (array.ndim - 1 - axis_at))

    one_side = jax.random.permutation(key, parts)[block_of(target)]
    other_side = (block_of(target) + parts // 2) % parts
    return jnp.where((block_of(source) == one_side) | (block_of(source) == other_side), factor * array, array)


def steps_of(key, extent, shards, smallest, top_value):
    gain, own = 1.0, jax.random.fold_in(key, 6)
    for dim, parts in shards:
        steps = jnp.exp(jax.random.uniform(jax.random.fold_in(own, dim), (parts,), jnp.float32, smallest / len(shards), top_value / len(shards)))
        gain = gain * jnp.repeat(steps, extent[dim] // parts).reshape([-1 if axis == dim else 1 for axis in range(len(extent))])
    return gain


def shared_out(rng, own, number, rows, count, top, limit, slope):
    ranking = jax.random.permutation(rng, count)
    packed, ordinary = portions_of(count, rows * top, limit, slope, True), portions_of(count, rows * top, limit, slope, False)
    places = jnp.arange(count)

    def named(lengths, turn):
        used = int((lengths > 0).sum())
        fixed = max(1, used // 4)
        shifted = fixed + (places - fixed + turn * (used - fixed)) % max(1, count - fixed)
        return jnp.zeros((count,), jnp.int32).at[ranking[jnp.where(places < fixed, places, shifted)]].set(jnp.asarray(lengths, jnp.int32))

    lengths = jnp.where(number % 4 == 0, named(packed, number // 4), named(ordinary, number - number // 4 - 1))
    mixed = jax.random.permutation(jax.random.fold_in(own, 3), count)
    source_of, sink = mixed[0:count // 2 * 2:2], mixed[1:count // 2 * 2:2]
    room = jnp.minimum(lengths[source_of] - 1, limit - lengths[sink]) // 2
    room = jnp.where((source_of == ranking[0]) | (sink == ranking[0]) | (lengths[sink] == 0), 0, jnp.maximum(room, 0))
    shifted = jax.random.randint(jax.random.fold_in(own, 4), (count // 2,), 0, 1 << 20) % (room + 1)
    lengths = lengths.at[source_of].add(-shifted).at[sink].add(shifted)
    members = jnp.searchsorted(jnp.cumsum(lengths), jnp.arange(rows * top), side="right").astype(jnp.int32)
    grid = members.reshape(top, rows).T
    grid = grid[jax.random.permutation(jax.random.fold_in(own, 1), rows)]
    turn = jax.random.randint(jax.random.fold_in(own, 2), (rows, 1), 0, top)
    return jnp.take_along_axis(grid, (jnp.arange(top)[None, :] + turn) % top, axis=1)


def portions_of(amount, total, bound, lean, full):
    loads = [(1 << 20) // math.isqrt(standing ** lean) + 1 for standing in range(1, amount + 1)]
    largest = bound if full else min(bound, max(-(-total // amount), total * loads[0] // sum(loads)))
    least = 1 if total - largest >= amount - 1 else 0
    given, spare = [largest] + [least] * (amount - 1), total - largest - least * (amount - 1)
    while spare > 0:
        candidates = [i for i in range(1, amount) if given[i] < largest] or [i for i in range(1, amount) if given[i] < bound]
        mass, left = sum([loads[i] for i in candidates]), spare
        for i in candidates:
            extra = min(bound - given[i], max(1, left * loads[i] // mass), spare)
            given[i] = given[i] + extra
            spare = spare - extra
    return np.array(given)


def gaussian(stream_key, extent, spread, limit, pieces=(), kind=jnp.bfloat16):
    loudness = steps_of(stream_key, extent, pieces, -0.22, 0.18) if pieces else 1.0
    result = jax.random.normal(stream_key, extent, jnp.float32) * spread * loudness
    return jnp.minimum(jnp.maximum(result, -limit), limit).astype(kind)


def noise_with(own_key, extent, scale, bound, pieces, heavy, kind=jnp.bfloat16):
    entries = scale * jax.random.normal(own_key, extent, jnp.float32)
    if pieces:
        entries = entries * steps_of(own_key, extent, pieces, -0.22, 0.18)
    return jnp.clip(spiked(entries, jax.random.fold_in(own_key, 3), *heavy), -bound, bound).astype(kind)


def setup_inputs(seed: int = 0) -> dict:
    splits = jax.random.split(jax.random.key(seed), 14)
    stream = draw_stream(jax.random.fold_in(splits[13], 71), 0)
    norm_gain = jnp.clip(1.0 + 0.18 * jax.random.normal(splits[1], (D,), jnp.float32), 0.1, 1.9)
    cotangent = noise_with(splits[2], (TOKENS, D), 1.0, 16.0, ((0, 64), (1, 2)), (0, 1, 64, 4.0))
    route_weights = jnp.clip(0.1 + 1.4 * jax.random.uniform(splits[3], (TOKENS, K), jnp.float32) ** steps_of(splits[3], (TOKENS, K), ((0, 64),), -0.2, 0.2), 0.1, 1.5)
    routes_keys = jax.random.split(jax.random.fold_in(splits[4], 1), TOKENS // TOK_DEV)
    routes_turns = jax.random.permutation(jax.random.fold_in(splits[4], 3), TOKENS // TOK_DEV)
    routes = jax.vmap(lambda own, number: shared_out(jax.random.fold_in(splits[4], 2), own, number, TOK_DEV, EXPERTS, K, CAP, 1))(routes_keys, routes_turns).reshape((TOKENS, K))
    conv_input = gaussian(splits[5], (TOKENS, CW), 1.0, 6.0, ((0, 64), (1, 2)))
    conv_bgate = gaussian(splits[6], (TOKENS, CW), 1.0, 6.0, ((0, 64), (1, 2)))
    conv_cgate = gaussian(splits[7], (TOKENS, CW), 1.0, 6.0, ((0, 64), (1, 2)))
    conv_taps = gaussian(splits[8], (3, CW), 0.5, 3.0, ((1, 2),), jnp.float32)
    out_proj = gaussian(splits[9], (D, CW), CW ** -0.5, 0.1875, ((1, 2),))
    gate_weight = gaussian(splits[10], (EXPERTS, D, EH), D ** -0.5, 0.125, ((0, 64), (2, 2)))
    up_weight = gaussian(splits[11], (EXPERTS, D, EH), D ** -0.5, 0.125, ((0, 64), (2, 2)))
    down_weight = gaussian(splits[12], (EXPERTS, EH, D), EH ** -0.5, 0.1875, ((0, 64), (1, 2)))
    return {"stream": stream, "norm_gain": norm_gain, "cotangent": cotangent, "route_weights": route_weights, "routes": routes, "conv_input": conv_input, "conv_bgate": conv_bgate, "conv_cgate": conv_cgate, "conv_taps": conv_taps, "out_proj": out_proj, "gate_weight": gate_weight, "up_weight": up_weight, "down_weight": down_weight}


EPSILON = 1e-06

def expert_backward(inputs, grads_out, gate_w, up_w, down_w):
    gate_lin = jnp.dot(inputs, gate_w, preferred_element_type=jnp.float32)
    up_lin = jnp.dot(inputs, up_w, preferred_element_type=jnp.float32)
    sigmoid_gate = jax.nn.sigmoid(gate_lin)
    silu_gate = gate_lin * sigmoid_gate
    hidden = (silu_gate * up_lin).astype(jnp.bfloat16)
    down_g = jnp.dot(hidden.T, grads_out, preferred_element_type=jnp.float32)
    hidden_grad = jnp.dot(grads_out, down_w.T, preferred_element_type=jnp.float32)
    gate_pre = (hidden_grad * up_lin * sigmoid_gate * (1.0 + gate_lin * (1.0 - sigmoid_gate))).astype(jnp.bfloat16)
    up_pre = (hidden_grad * silu_gate).astype(jnp.bfloat16)
    gate_g = jnp.dot(inputs.T, gate_pre, preferred_element_type=jnp.float32)
    up_g = jnp.dot(inputs.T, up_pre, preferred_element_type=jnp.float32)
    return (gate_g, up_g, down_g, gate_pre, up_pre)

def reference(stream, norm_gain, cotangent, route_weights, routes, conv_input, conv_bgate, conv_cgate, conv_taps, out_proj, gate_weight, up_weight, down_weight):
    stream_float = stream.astype(jnp.float32)
    inverse = lax.rsqrt(lax.optimization_barrier(jnp.mean(stream_float * stream_float, axis=1, keepdims=True)) + EPSILON)
    normed = (stream_float * inverse * norm_gain[None, :]).astype(jnp.bfloat16)
    cot_float = cotangent.astype(jnp.float32)
    weighted = (route_weights[:, :, None] * cot_float[:, None, :]).astype(jnp.bfloat16).reshape(TOKENS * K, D)
    blocks = routes.reshape(N_SP, TOK_DEV * K).astype(jnp.int32)
    onehot = (blocks[:, :, None] == jnp.arange(EXPERTS, dtype=jnp.int32)[None, None, :]).astype(jnp.int32)
    earlier = jnp.cumsum(onehot, axis=1) - onehot
    position = lax.optimization_barrier(jnp.sum(earlier * onehot, axis=2)).astype(jnp.int32)
    source = jnp.arange(N_SP, dtype=jnp.int32)[:, None]
    arrival = (source * CAP + position).astype(jnp.int32)
    assign_ids = jnp.arange(TOKENS * K, dtype=jnp.int32).reshape(N_SP, TOK_DEV * K)
    table = jnp.full((EXPERTS, N_SP * CAP), TOKENS * K, jnp.int32).at[blocks, arrival].set(assign_ids)
    normed_pad = jnp.concatenate([normed, jnp.zeros((1, D), jnp.bfloat16)], axis=0)
    weighted_pad = jnp.concatenate([weighted, jnp.zeros((1, D), jnp.bfloat16)], axis=0)
    half_width = EH // N_TP

    def one_expert(operands):
        slot_ids, gate_w, up_w, down_w = operands
        token_ids = (slot_ids // K).astype(jnp.int32)
        inputs = normed_pad[token_ids]
        grads_out = weighted_pad[slot_ids]
        gate_g, up_g, down_g, gate_pre, up_pre = expert_backward(inputs, grads_out, gate_w, up_w, down_w)
        summed = jnp.zeros((N_SP * CAP, D), jnp.float32)
        for part_index in range(N_TP):
            low_col = part_index * half_width
            partial_value = jnp.dot(gate_pre[:, low_col:low_col + half_width], gate_w[:, low_col:low_col + half_width].T, preferred_element_type=jnp.float32)
            partial_value = partial_value + jnp.dot(up_pre[:, low_col:low_col + half_width], up_w[:, low_col:low_col + half_width].T, preferred_element_type=jnp.float32)
            rounded = lax.optimization_barrier(partial_value.astype(jnp.bfloat16))
            summed = summed + rounded.astype(jnp.float32)
        return (gate_g, up_g, down_g, summed.astype(jnp.bfloat16))
    gate_grad, up_grad, down_grad, slot_grads = lax.map(one_expert, (table, gate_weight, up_weight, down_weight))
    token_index = (table.reshape(-1) // K).astype(jnp.int32)
    normed_grad = jnp.zeros((TOKENS + 1, D), jnp.float32).at[token_index].add(slot_grads.reshape(-1, D).astype(jnp.float32))[:TOKENS]
    cross = lax.optimization_barrier(jnp.sum(stream_float * norm_gain[None, :] * normed_grad, axis=1, keepdims=True))
    stream_grad = (cot_float + inverse * norm_gain[None, :] * normed_grad - stream_float * inverse * inverse * inverse * cross / D).astype(jnp.bfloat16)
    input_float = conv_input.astype(jnp.float32)
    cgate_float = conv_cgate.astype(jnp.float32)
    bgate_float = conv_bgate.astype(jnp.float32)
    gated = cgate_float * input_float
    padded = jnp.pad(gated, ((2, 0), (0, 0)))
    conv_out = conv_taps[0][None, :] * padded[:-2] + conv_taps[1][None, :] * padded[1:-1] + conv_taps[2][None, :] * padded[2:]
    mixer_out = (bgate_float * conv_out).astype(jnp.bfloat16)
    proj_grad = lax.dot_general(stream_grad, mixer_out, (((0,), (0,)), ((), ())), preferred_element_type=jnp.float32)
    mixer_grad = jnp.dot(stream_grad, out_proj, preferred_element_type=jnp.float32)
    delta = mixer_grad * bgate_float
    padded_back = jnp.pad(delta, ((0, 2), (0, 0)))
    gated_grad = conv_taps[2][None, :] * padded_back[:-2] + conv_taps[1][None, :] * padded_back[1:-1] + conv_taps[0][None, :] * padded_back[2:]
    bgate_grad = (mixer_grad * conv_out).astype(jnp.bfloat16)
    input_grad = (gated_grad * cgate_float).astype(jnp.bfloat16)
    cgate_grad = (gated_grad * input_float).astype(jnp.bfloat16)
    return (stream_grad, proj_grad, input_grad, bgate_grad, cgate_grad, gate_grad, up_grad, down_grad)
```

```python
import jax
import jax.numpy as jnp
from jax import lax
from jax.experimental import pallas as pl
from jax.experimental.pallas import tpu as pltpu
from jax.sharding import Mesh
from jax.sharding import PartitionSpec as P

D = 2048
SP = ("sp_0", "sp_1", "sp_2")
EPSILON = 1e-06
VMEM = 56 * 1024 * 1024
F32 = jnp.float32
BF16 = jnp.bfloat16


def dot_nn(a, b):
    return lax.dot_general(a, b, (((1,), (0,)), ((), ())), preferred_element_type=F32)


def dot_nt(a, b):
    return lax.dot_general(a, b, (((1,), (1,)), ((), ())), preferred_element_type=F32)


def dot_tn(a, b):
    return lax.dot_general(a, b, (((0,), (0,)), ((), ())), preferred_element_type=F32)


def cost(flops, size):
    return pl.CostEstimate(flops=flops, transcendentals=0, bytes_accessed=size)


def swap(value):
    return lax.ppermute(value, "tp", [(0, 1), (1, 0)])


def exchange(value, axis):
    return lax.all_to_all(value, axis, split_axis=0, concat_axis=0, tiled=True)


def shifted(value, axis, steps):
    count = lax.axis_size(axis)
    leading, last = (max(0, -steps), min(count, count - steps))
    return lax.ppermute(value, axis, [(source, source + steps) for source in range(leading, last)])


def turned(value, axis, steps):
    count = lax.axis_size(axis)
    return lax.ppermute(value, axis, [(i, (i + steps) % count) for i in range(count)])


def slots_body(experts, capacity, stream_ref, routes_ref, squares_ref, target_ref):
    values = stream_ref[...].astype(F32)
    squares = values * values
    high = squares.astype(BF16)
    low = (squares - high.astype(F32)).astype(BF16)
    ones = jnp.ones((8, values.shape[1]), BF16)
    squares_ref[...] = (dot_nt(ones, high) + dot_nt(ones, low))[0:1]
    tokens = values.shape[0]
    first, second = routes_ref[0:1, :], routes_ref[1:2, :]
    ids = lax.broadcasted_iota(jnp.int32, (experts, tokens), 0)
    named_first = (ids == first).astype(F32)
    named_second = (ids == second).astype(F32)
    before = (
        lax.broadcasted_iota(jnp.int32, (tokens, tokens), 0)
        < lax.broadcasted_iota(jnp.int32, (tokens, tokens), 1)
    ).astype(F32)
    earlier = dot_nn((named_first + named_second).astype(BF16), before.astype(BF16))
    rank_first = jnp.sum(named_first * earlier, axis=0, keepdims=True).astype(jnp.int32)
    rank_second = jnp.sum(named_second * earlier, axis=0, keepdims=True).astype(jnp.int32)
    target_ref[0:1, :] = first * capacity + rank_first
    target_ref[1:2, :] = second * capacity + rank_second


def find_slots(stream, routes, experts, capacity):
    tokens = stream.shape[0]

    def body(*refs):
        slots_body(experts, capacity, *refs)

    return pl.pallas_call(
        body,
        out_shape=(
            jax.ShapeDtypeStruct((1, tokens), F32),
            jax.ShapeDtypeStruct((2, tokens), jnp.int32),
        ),
        name="find_slots",
        cost_estimate=cost(10**8, stream.size * 2),
    )(stream, routes)


def rows_body(target_ref, weight_ref, total_ref, stream_ref, cot_ref, gain_ref, out_ref, sel_ref):
    rows, tokens = sel_ref.shape
    width = stream_ref.shape[1]
    slots = lax.broadcasted_iota(jnp.int32, (rows, tokens), 0) + pl.program_id(0) * rows
    first = slots == target_ref[0:1, :]
    second = slots == target_ref[1:2, :]
    inverse = lax.rsqrt(total_ref[...] / D + EPSILON)
    both = jnp.where(first | second, 1.0, 0.0)
    selector = both.astype(BF16)
    scale = jnp.sum(both * inverse, axis=1, keepdims=True)
    weight = jnp.where(first, weight_ref[0:1, :], 0.0) + jnp.where(second, weight_ref[1:2, :], 0.0)
    weight = jnp.sum(weight, axis=1, keepdims=True)
    sel_ref[...] = selector
    inputs = dot_nn(selector, stream_ref[...])
    out_ref[:, :width] = (inputs * scale * gain_ref[...]).astype(BF16)
    grads = dot_nn(selector, cot_ref[...])
    out_ref[:, width:] = (weight * grads).astype(BF16)


def build_rows(target, weights, total, stream, cot, gain, slots):
    tokens, width = stream.shape
    rows = slots // 8

    def whole(*shape):
        return pl.BlockSpec(shape, lambda i: (0, 0))

    return pl.pallas_call(
        rows_body,
        grid=(8,),
        in_specs=[
            whole(2, tokens),
            whole(2, tokens),
            whole(1, tokens),
            whole(tokens, width),
            whole(tokens, width),
            whole(1, width),
        ],
        out_specs=(
            pl.BlockSpec((rows, 2 * width), lambda i: (i, 0)),
            pl.BlockSpec((rows, tokens), lambda i: (i, 0)),
        ),
        out_shape=(
            jax.ShapeDtypeStruct((slots, 2 * width), BF16),
            jax.ShapeDtypeStruct((slots, tokens), BF16),
        ),
        name="build_rows",
        cost_estimate=cost(4 * slots * tokens * width, slots * width * 4),
    )(target, weights, total, stream, cot, gain)


def expert_body(
    core_ref, own_ref, peer_ref, gate_own, gate_peer, up_own, up_peer, down_own, down_peer,
    hidden_ref, gate_ref, up_ref, mine_ref, theirs_ref,
):
    width = gate_own.shape[0]
    own_x, own_y = own_ref[:, :width], own_ref[:, width:]
    peer_x, peer_y = peer_ref[:, :width], peer_ref[:, width:]
    gate_lin = dot_nn(own_x, gate_own[...]) + dot_nn(peer_x, gate_peer[...])
    up_lin = dot_nn(own_x, up_own[...]) + dot_nn(peer_x, up_peer[...])
    hidden_grad = dot_nt(own_y, down_own[...]) + dot_nt(peer_y, down_peer[...])
    sig = jax.nn.sigmoid(gate_lin)
    silu = gate_lin * sig
    hidden_ref[...] = (silu * up_lin).astype(BF16)
    gate_pre = (hidden_grad * up_lin * sig * (1.0 + gate_lin * (1.0 - sig))).astype(BF16)
    up_pre = (hidden_grad * silu).astype(BF16)
    gate_ref[...] = gate_pre
    up_ref[...] = up_pre
    mine_ref[...] = (dot_nt(gate_pre, gate_own[...]) + dot_nt(up_pre, up_own[...])).astype(BF16)
    theirs_ref[...] = (dot_nt(gate_pre, gate_peer[...]) + dot_nt(up_pre, up_peer[...])).astype(BF16)


def expert_rows(core, own, peer, gate_w, up_w, down_w):
    rows, double = own.shape
    width = double // 2
    units = gate_w.shape[1]
    step = 256

    def block(n):
        return pl.BlockSpec((step, n), lambda i, c: (i, 0))

    tall_own = pl.BlockSpec((width, units), lambda i, c: (c[0], 0))
    tall_peer = pl.BlockSpec((width, units), lambda i, c: (1 - c[0], 0))
    wide_own = pl.BlockSpec((units, width), lambda i, c: (0, c[0]))
    wide_peer = pl.BlockSpec((units, width), lambda i, c: (0, 1 - c[0]))
    narrow = jax.ShapeDtypeStruct((rows, units), BF16)
    broad = jax.ShapeDtypeStruct((rows, width), BF16)
    return pl.pallas_call(
        expert_body,
        grid_spec=pltpu.PrefetchScalarGridSpec(
            num_scalar_prefetch=1,
            grid=(rows // step,),
            in_specs=[
                block(double), block(double),
                tall_own, tall_peer, tall_own, tall_peer, wide_own, wide_peer,
            ],
            out_specs=[block(units), block(units), block(units), block(width), block(width)],
        ),
        out_shape=[narrow, narrow, narrow, broad, broad],
        compiler_params=pltpu.CompilerParams(vmem_limit_bytes=VMEM),
        name="expert_rows",
        cost_estimate=cost(20 * rows * width * units, 20 * rows * width),
    )(core, own, peer, gate_w, gate_w, up_w, up_w, down_w, down_w)


def weights_body(
    core_ref, own_x, own_y, peer_x, peer_y, hidden_ref, gate_ref, up_ref,
    gate_out, up_out, down_out,
):
    def emit(x, y):
        gate_out[...] = dot_tn(x, gate_ref[...])
        up_out[...] = dot_tn(x, up_ref[...])
        down_out[...] = dot_tn(hidden_ref[...], y)

    half = pl.num_programs(0) // 2

    @pl.when(pl.program_id(0) < half)
    def _():
        emit(own_x[...], own_y[...])

    @pl.when(pl.program_id(0) >= half)
    def _():
        emit(peer_x[...], peer_y[...])


def weight_grads(core, own, peer, hidden, gate_pre, up_pre):
    rows, double = own.shape
    width = double // 2
    units = hidden.shape[1]
    chunk = 256
    half = width // chunk

    def own_at(base):
        return pl.BlockSpec((rows, chunk), lambda s, c: (0, base + jnp.minimum(s, half - 1)))

    def peer_at(base):
        return pl.BlockSpec((rows, chunk), lambda s, c: (0, base + jnp.maximum(s - half, 0)))

    def place(s, c):
        side = jnp.where(s < half, c[0], 1 - c[0])
        return side * half + jnp.where(s < half, s, s - half)

    whole = pl.BlockSpec((rows, units), lambda s, c: (0, 0))
    tall = pl.BlockSpec((chunk, units), lambda s, c: (place(s, c), 0))
    wide = pl.BlockSpec((units, chunk), lambda s, c: (0, place(s, c)))
    return pl.pallas_call(
        weights_body,
        grid_spec=pltpu.PrefetchScalarGridSpec(
            num_scalar_prefetch=1,
            grid=(2 * half,),
            in_specs=[own_at(0), own_at(half), peer_at(0), peer_at(half), whole, whole, whole],
            out_specs=[tall, tall, wide],
        ),
        out_shape=[
            jax.ShapeDtypeStruct((double, units), F32),
            jax.ShapeDtypeStruct((double, units), F32),
            jax.ShapeDtypeStruct((units, double), F32),
        ],
        compiler_params=pltpu.CompilerParams(vmem_limit_bytes=VMEM),
        name="weight_grads",
        cost_estimate=cost(12 * rows * width * units, 24 * width * units),
    )(core, own, own, peer, peer, hidden, gate_pre, up_pre)


def local(
    stream,
    norm_gain,
    cotangent,
    route_weights,
    routes,
    conv_input,
    conv_bgate,
    conv_cgate,
    conv_taps,
    out_proj,
    gate_weight,
    up_weight,
    down_weight,
):
    experts = lax.axis_size(SP)
    tok_count, width = stream.shape
    top_count = routes.shape[1]
    capacity = 2 * tok_count * top_count // experts
    slots = experts * capacity
    core = lax.axis_index("tp")
    core_arg = core.astype(jnp.int32).reshape(1)
    gain_row = norm_gain[None, :]

    squares, target = find_slots(stream, routes.T, experts, capacity)
    total = squares + swap(squares)
    rows, selector = build_rows(
        target, route_weights.T, total, stream, cotangent, gain_row, slots
    )
    own = exchange(rows.reshape(experts, capacity, 2 * width), SP).reshape(slots, 2 * width)

    input_float = conv_input.astype(F32)
    cgate_float = conv_cgate.astype(F32)
    bgate_float = conv_bgate.astype(F32)
    rim_rows = shifted(jnp.stack([conv_input[-2:], conv_cgate[-2:]]), SP, 1)
    rim_gated = rim_rows[1].astype(F32) * rim_rows[0].astype(F32)
    gated = cgate_float * input_float
    extended = jnp.concatenate([rim_gated, gated], axis=0)
    conv_out = (
        conv_taps[0][None, :] * extended[:-2]
        + conv_taps[1][None, :] * extended[1:-1]
        + conv_taps[2][None, :] * extended[2:]
    )
    mixer_out = (bgate_float * conv_out).astype(BF16)
    line = lax.axis_size("sp_0")
    spot = lax.axis_index("sp_0")
    around = jnp.stack([mixer_out] + [turned(mixer_out, "sp_0", s) for s in range(1, line)])
    mixers = jnp.concatenate(
        [lax.dynamic_slice_in_dim(around, (spot - k) % line, 1, 0) for k in range(line)], axis=0
    )
    token_half = tok_count // 2
    channels = mixer_out.shape[1]

    def half_of(array, which, dim):
        return lax.dynamic_slice_in_dim(array, which * token_half, token_half, dim)

    mixers_mine = half_of(mixers, core, 1).reshape(line * token_half, channels)
    mixers_theirs = half_of(mixers, 1 - core, 1).reshape(line * token_half, channels)

    peer = swap(own)
    hidden, gate_pre, up_pre, part_mine, part_theirs = expert_rows(
        core_arg, own, peer, gate_weight[0], up_weight[0], down_weight[0]
    )
    other = swap(part_theirs)
    row_grads = (part_mine.astype(F32) + other.astype(F32)).astype(BF16)
    returned = exchange(row_grads.reshape(experts, capacity, width), SP).reshape(slots, width)
    gate_g, up_g, down_g = weight_grads(core_arg, own, peer, hidden, gate_pre, up_pre)

    normed_grad = dot_tn(selector, returned)
    stream_float = stream.astype(F32)
    cot_float = cotangent.astype(F32)
    inverse = lax.rsqrt(total[0] / D + EPSILON)[:, None]
    cross_part = jnp.sum(stream_float * gain_row * normed_grad, axis=1)
    cross = cross_part + swap(cross_part)
    stream_grad = (
        cot_float
        + inverse * gain_row * normed_grad
        - stream_float * inverse * inverse * inverse * cross[:, None] / D
    ).astype(BF16)

    grad_peer = swap(stream_grad)
    mine_half, peer_half = half_of(stream_grad, core, 0), half_of(grad_peer, core, 0)
    low = jnp.where(core == 0, mine_half, peer_half)
    high = jnp.where(core == 0, peer_half, mine_half)
    quarter = 2 * width // line
    parts = [low[:, :quarter], low[:, quarter:], high[:, :quarter], high[:, quarter:]]
    sent = jnp.stack(parts)
    grads_mine = exchange(sent, "sp_0").reshape(line * token_half, quarter)
    grads_theirs = swap(grads_mine)
    proj_part = dot_tn(grads_mine, mixers_mine) + dot_tn(grads_theirs, mixers_theirs)
    plane = lax.axis_size(("sp_1", "sp_2"))
    arrived = exchange(proj_part.reshape(plane, quarter // plane, channels), ("sp_1", "sp_2"))
    proj_grad = arrived.sum(axis=0)

    proj_mine = lax.dynamic_slice_in_dim(out_proj, core * width, width, 0)
    proj_peer = lax.dynamic_slice_in_dim(out_proj, (1 - core) * width, width, 0)
    mixer_grad = dot_nn(stream_grad, proj_mine) + dot_nn(grad_peer, proj_peer)
    delta = mixer_grad * bgate_float
    next_rim = shifted(delta[:2], SP, -1)
    extended_back = jnp.concatenate([delta, next_rim], axis=0)
    gated_grad = (
        conv_taps[2][None, :] * extended_back[:-2]
        + conv_taps[1][None, :] * extended_back[1:-1]
        + conv_taps[0][None, :] * extended_back[2:]
    )
    bgate_grad = (mixer_grad * conv_out).astype(BF16)
    input_grad = (gated_grad * cgate_float).astype(BF16)
    cgate_grad = (gated_grad * input_float).astype(BF16)
    return (
        stream_grad,
        proj_grad,
        input_grad,
        bgate_grad,
        cgate_grad,
        gate_g[None],
        up_g[None],
        down_g[None],
    )


def solution(mesh):
    finer = Mesh(mesh.devices.reshape(4, 4, 4, mesh.shape["tp"]), ("sp_0", "sp_1", "sp_2", "tp"))
    return jax.shard_map(
        local,
        mesh=finer,
        in_specs=(
            P(SP, "tp"),
            P("tp"),
            P(SP, "tp"),
            P(SP, None),
            P(SP, None),
            P(SP, "tp"),
            P(SP, "tp"),
            P(SP, "tp"),
            P(None, "tp"),
            P(None, "tp"),
            P(SP, None, "tp"),
            P(SP, None, "tp"),
            P(SP, "tp", None),
        ),
        out_specs=(
            P(SP, "tp"),
            P(SP, "tp"),
            P(SP, "tp"),
            P(SP, "tp"),
            P(SP, "tp"),
            P(SP, None, "tp"),
            P(SP, None, "tp"),
            P(SP, "tp", None),
        ),
        check_vma=False,
    )
```

```python
import jax
import jax.numpy as jnp
from jax import lax
from jax.experimental import pallas as pl
from jax.experimental.pallas import tpu as pltpu
from jax.sharding import Mesh
from jax.sharding import PartitionSpec as P


D = 2048
SP = ("sp_0", "sp_1", "sp_2")
EPSILON = 1e-06
VMEM = 56 * 1024 * 1024
EXPERT_BLOCKS = 2
F32 = jnp.float32
BF16 = jnp.bfloat16


def dot_nn(a, b):
    return lax.dot_general(a, b, (((1,), (0,)), ((), ())), preferred_element_type=F32)


def dot_nt(a, b):
    return lax.dot_general(a, b, (((1,), (1,)), ((), ())), preferred_element_type=F32)


def dot_tn(a, b):
    return lax.dot_general(a, b, (((0,), (0,)), ((), ())), preferred_element_type=F32)


def cost(flops, size):
    return pl.CostEstimate(flops=flops, transcendentals=0, bytes_accessed=size)


def swap(value):
    return lax.ppermute(value, "tp", [(0, 1), (1, 0)])


def exchange(value, axis):
    return lax.all_to_all(value, axis, split_axis=0, concat_axis=0, tiled=True)


def shifted(value, axis, steps):
    count = lax.axis_size(axis)
    leading, last = (max(0, -steps), min(count, count - steps))
    return lax.ppermute(value, axis, [(source, source + steps) for source in range(leading, last)])


def turned(value, axis, steps):
    count = lax.axis_size(axis)
    return lax.ppermute(value, axis, [(i, (i + steps) % count) for i in range(count)])


def slots_body(experts, capacity, stream_ref, routes_ref, squares_ref, target_ref):
    values = stream_ref[...].astype(F32)
    squares = values * values
    high = squares.astype(BF16)
    low = (squares - high.astype(F32)).astype(BF16)
    ones = jnp.ones((8, values.shape[1]), BF16)
    squares_ref[...] = (dot_nt(ones, high) + dot_nt(ones, low))[0:1]
    tokens = values.shape[0]
    first, second = routes_ref[0:1, :], routes_ref[1:2, :]
    ids = lax.broadcasted_iota(jnp.int32, (experts, tokens), 0)
    named_first = (ids == first).astype(F32)
    named_second = (ids == second).astype(F32)
    before = (
        lax.broadcasted_iota(jnp.int32, (tokens, tokens), 0)
        < lax.broadcasted_iota(jnp.int32, (tokens, tokens), 1)
    ).astype(F32)
    earlier = dot_nn((named_first + named_second).astype(BF16), before.astype(BF16))
    rank_first = jnp.sum(named_first * earlier, axis=0, keepdims=True).astype(jnp.int32)
    rank_second = jnp.sum(named_second * earlier, axis=0, keepdims=True).astype(jnp.int32)
    target_ref[0:1, :] = first * capacity + rank_first
    target_ref[1:2, :] = second * capacity + rank_second


def find_slots(stream, routes, experts, capacity):
    tokens = stream.shape[0]

    def body(*refs):
        slots_body(experts, capacity, *refs)

    return pl.pallas_call(
        body,
        out_shape=(
            jax.ShapeDtypeStruct((1, tokens), F32),
            jax.ShapeDtypeStruct((2, tokens), jnp.int32),
        ),
        name="find_slots",
        cost_estimate=cost(10**8, stream.size * 2),
    )(stream, routes)


def rows_body(target_ref, weight_ref, total_ref, stream_ref, cot_ref, gain_ref, out_ref, sel_ref):
    rows, tokens = sel_ref.shape
    width = stream_ref.shape[1]
    slots = lax.broadcasted_iota(jnp.int32, (rows, tokens), 0) + pl.program_id(0) * rows
    first = slots == target_ref[0:1, :]
    second = slots == target_ref[1:2, :]
    inverse = lax.rsqrt(total_ref[...] / D + EPSILON)
    both = jnp.where(first | second, 1.0, 0.0)
    selector = both.astype(BF16)
    scale = jnp.sum(both * inverse, axis=1, keepdims=True)
    weight = jnp.where(first, weight_ref[0:1, :], 0.0) + jnp.where(second, weight_ref[1:2, :], 0.0)
    weight = jnp.sum(weight, axis=1, keepdims=True)
    sel_ref[...] = selector
    inputs = dot_nn(selector, stream_ref[...])
    out_ref[:, :width] = (inputs * scale * gain_ref[...]).astype(BF16)
    grads = dot_nn(selector, cot_ref[...])
    out_ref[:, width:] = (weight * grads).astype(BF16)


def build_rows(target, weights, total, stream, cot, gain, slots):
    tokens, width = stream.shape
    rows = slots // 4

    def whole(*shape):
        return pl.BlockSpec(shape, lambda i: (0, 0))

    return pl.pallas_call(
        rows_body,
        grid=(4,),
        in_specs=[
            whole(2, tokens),
            whole(2, tokens),
            whole(1, tokens),
            whole(tokens, width),
            whole(tokens, width),
            whole(1, width),
        ],
        out_specs=(
            pl.BlockSpec((rows, 2 * width), lambda i: (i, 0)),
            pl.BlockSpec((rows, tokens), lambda i: (i, 0)),
        ),
        out_shape=(
            jax.ShapeDtypeStruct((slots, 2 * width), BF16),
            jax.ShapeDtypeStruct((slots, tokens), BF16),
        ),
        name="build_rows",
        cost_estimate=cost(4 * slots * tokens * width, slots * width * 4),
    )(target, weights, total, stream, cot, gain)


def load_body(core_ref, gate_ref, up_ref, down_ref, *refs):
    outs, sems = refs[:6], refs[6]
    width = outs[0].shape[0]
    mine = pl.multiple_of(core_ref[0] * width, width)
    other = pl.multiple_of((1 - core_ref[0]) * width, width)
    sources = (
        gate_ref.at[pl.ds(mine, width), :],
        gate_ref.at[pl.ds(other, width), :],
        up_ref.at[pl.ds(mine, width), :],
        up_ref.at[pl.ds(other, width), :],
        down_ref.at[:, pl.ds(mine, width)],
        down_ref.at[:, pl.ds(other, width)],
    )
    copies = [
        pltpu.make_async_copy(source, outs[i], sems.at[i]) for i, source in enumerate(sources)
    ]
    for copy in copies:
        copy.start()
    for copy in copies:
        copy.wait()


def own_body(own_ref, gate_w, up_w, down_w, gate_out, up_out, hidden_out):
    rows, double = own_ref.shape
    width = double // 2
    step = rows // EXPERT_BLOCKS

    def block(i, carry):
        at = pl.ds(i * step, step)
        x, y = own_ref[at, :width], own_ref[at, width:]
        gate_out[at, :] = dot_nn(x, gate_w[...])
        up_out[at, :] = dot_nn(x, up_w[...])
        hidden_out[at, :] = dot_nt(y, down_w[...])
        return carry

    lax.fori_loop(0, EXPERT_BLOCKS, block, 0)


def peer_body(
    peer_ref, gate_w, up_w, down_w, gate_in, up_in, grad_in,
    hidden_ref, gate_ref, up_ref, theirs_ref,
):
    rows, double = peer_ref.shape
    width = double // 2
    step = rows // EXPERT_BLOCKS

    def block(i, carry):
        at = pl.ds(i * step, step)
        x, y = peer_ref[at, :width], peer_ref[at, width:]
        gate_lin = gate_in[at, :] + dot_nn(x, gate_w[...])
        up_lin = up_in[at, :] + dot_nn(x, up_w[...])
        hidden_grad = grad_in[at, :] + dot_nt(y, down_w[...])
        sig = jax.nn.sigmoid(gate_lin)
        silu = gate_lin * sig
        hidden_ref[at, :] = (silu * up_lin).astype(BF16)
        gate_pre = (hidden_grad * up_lin * sig * (1.0 + gate_lin * (1.0 - sig))).astype(BF16)
        up_pre = (hidden_grad * silu).astype(BF16)
        gate_ref[at, :] = gate_pre
        up_ref[at, :] = up_pre
        theirs_ref[at, :] = (dot_nt(gate_pre, gate_w[...]) + dot_nt(up_pre, up_w[...])).astype(BF16)
        return carry

    lax.fori_loop(0, EXPERT_BLOCKS, block, 0)


def mine_body(gate_ref, up_ref, gate_w, up_w, mine_ref):
    step = mine_ref.shape[0] // EXPERT_BLOCKS

    def block(i, carry):
        at = pl.ds(i * step, step)
        part = dot_nt(gate_ref[at, :], gate_w[...]) + dot_nt(up_ref[at, :], up_w[...])
        mine_ref[at, :] = part.astype(BF16)
        return carry

    lax.fori_loop(0, EXPERT_BLOCKS, block, 0)


def add_body(mine_ref, other_ref, out_ref, scratch, sems):
    blocks, step, _ = scratch.shape
    copies = []
    for i in range(blocks):
        at = pl.ds(i * step, step)
        total = mine_ref[at, :].astype(F32) + other_ref[at, :].astype(F32)
        scratch[i] = total.astype(BF16)
        copies.append(pltpu.make_async_copy(scratch.at[i], out_ref.at[at, :], sems.at[i]))
        copies[-1].start()
    for copy in copies:
        copy.wait()


IN_VMEM = pl.BlockSpec(memory_space=pltpu.VMEM)


def on_chip(body, outs, flops, limit, *args):
    return pl.pallas_call(
        body,
        in_specs=[IN_VMEM] * len(args),
        out_specs=[IN_VMEM] * len(outs),
        out_shape=[jax.ShapeDtypeStruct(s, d) for s, d in outs],
        compiler_params=pltpu.CompilerParams(vmem_limit_bytes=limit * 1024 * 1024),
        cost_estimate=cost(flops, 16 * 1024 * 1024),
    )(*args)


def load_weights(core, gate_w, up_w, down_w):
    double, units = gate_w.shape
    width = double // 2
    shapes = [(width, units)] * 4 + [(units, width)] * 2
    return pl.pallas_call(
        load_body,
        in_specs=[pl.BlockSpec(memory_space=pltpu.SMEM)] + [pl.BlockSpec(memory_space=pl.ANY)] * 3,
        out_specs=[IN_VMEM] * 6,
        out_shape=[jax.ShapeDtypeStruct(s, BF16) for s in shapes],
        scratch_shapes=[pltpu.SemaphoreType.DMA((6,))],
        name="load_weights",
        cost_estimate=cost(10**9, 6 * double * units),
    )(core, gate_w, up_w, down_w)


def expert_own(own, gate_w, up_w, down_w):
    rows, units = own.shape[0], gate_w.shape[1]
    outs = [((rows, units), F32)] * 3
    flops = 3 * rows * own.shape[1] * units
    return on_chip(own_body, outs, flops, 8, own, gate_w, up_w, down_w)


def expert_peer(peer, gate_w, up_w, down_w, *parts):
    rows, units = peer.shape[0], gate_w.shape[1]
    outs = [((rows, units), BF16)] * 3 + [((rows, peer.shape[1] // 2), BF16)]
    flops = 5 * rows * peer.shape[1] * units
    return on_chip(peer_body, outs, flops, 16, peer, gate_w, up_w, down_w, *parts)


def expert_mine(gate_pre, up_pre, gate_w, up_w):
    rows, width = gate_pre.shape[0], gate_w.shape[0]
    flops = 4 * rows * width * gate_w.shape[1]
    outs = [((rows, width), BF16)]
    return on_chip(mine_body, outs, flops, 8, gate_pre, up_pre, gate_w, up_w)[0]


def add_parts(mine, other):
    rows, width = mine.shape
    blocks = 8
    return pl.pallas_call(
        add_body,
        in_specs=[IN_VMEM] * 2,
        out_specs=pl.BlockSpec(memory_space=pltpu.HBM),
        out_shape=jax.ShapeDtypeStruct(mine.shape, BF16),
        scratch_shapes=[
            pltpu.VMEM((blocks, rows // blocks, width), BF16),
            pltpu.SemaphoreType.DMA((blocks,)),
        ],
        compiler_params=pltpu.CompilerParams(vmem_limit_bytes=8 * 1024 * 1024),
        name="add_parts",
        cost_estimate=cost(mine.size, 6 * mine.size),
    )(mine, other)


def weights_body(
    core_ref, own_x, own_y, peer_x, peer_y, hidden_ref, gate_ref, up_ref,
    gate_out, up_out, down_out,
):
    def emit(x, y):
        gate_out[...] = dot_tn(x, gate_ref[...])
        up_out[...] = dot_tn(x, up_ref[...])
        down_out[...] = dot_tn(hidden_ref[...], y)

    half = pl.num_programs(0) // 2

    @pl.when(pl.program_id(0) < half)
    def _():
        emit(own_x[...], own_y[...])

    @pl.when(pl.program_id(0) >= half)
    def _():
        emit(peer_x[...], peer_y[...])


def weight_grads(core, own, peer, hidden, gate_pre, up_pre):
    rows, double = own.shape
    width = double // 2
    units = hidden.shape[1]
    chunk = 256
    half = width // chunk

    def own_at(base):
        return pl.BlockSpec((rows, chunk), lambda s, c: (0, base + jnp.minimum(s, half - 1)))

    def peer_at(base):
        return pl.BlockSpec((rows, chunk), lambda s, c: (0, base + jnp.maximum(s - half, 0)))

    def place(s, c):
        side = jnp.where(s < half, c[0], 1 - c[0])
        return side * half + jnp.where(s < half, s, s - half)

    whole = pl.BlockSpec((rows, units), lambda s, c: (0, 0))
    tall = pl.BlockSpec((chunk, units), lambda s, c: (place(s, c), 0))
    wide = pl.BlockSpec((units, chunk), lambda s, c: (0, place(s, c)))
    return pl.pallas_call(
        weights_body,
        grid_spec=pltpu.PrefetchScalarGridSpec(
            num_scalar_prefetch=1,
            grid=(2 * half,),
            in_specs=[own_at(0), own_at(half), peer_at(0), peer_at(half), whole, whole, whole],
            out_specs=[tall, tall, wide],
        ),
        out_shape=[
            jax.ShapeDtypeStruct((double, units), F32),
            jax.ShapeDtypeStruct((double, units), F32),
            jax.ShapeDtypeStruct((units, double), F32),
        ],
        compiler_params=pltpu.CompilerParams(vmem_limit_bytes=VMEM),
        name="weight_grads",
        cost_estimate=cost(12 * rows * width * units, 24 * width * units),
    )(core, own, own, peer, peer, hidden, gate_pre, up_pre)


def stage(
    stream,
    norm_gain,
    cotangent,
    route_weights,
    routes,
    conv_input,
    conv_bgate,
    conv_cgate,
    conv_taps,
    out_proj,
    gate_weight,
    up_weight,
    down_weight,
):
    experts = lax.axis_size(SP)
    tok_count, width = stream.shape
    top_count = routes.shape[1]
    capacity = 2 * tok_count * top_count // experts
    slots = experts * capacity
    core = lax.axis_index("tp")
    core_arg = core.astype(jnp.int32).reshape(1)
    gain_row = norm_gain[None, :]

    squares, target = find_slots(stream, routes.T, experts, capacity)
    total = squares + swap(squares)
    rows, selector = build_rows(
        target, route_weights.T, total, stream, cotangent, gain_row, slots
    )
    own = exchange(rows.reshape(experts, capacity, 2 * width), SP).reshape(slots, 2 * width)

    input_float = conv_input.astype(F32)
    cgate_float = conv_cgate.astype(F32)
    bgate_float = conv_bgate.astype(F32)
    rim_rows = shifted(jnp.stack([conv_input[-2:], conv_cgate[-2:]]), SP, 1)
    rim_gated = rim_rows[1].astype(F32) * rim_rows[0].astype(F32)
    gated = cgate_float * input_float
    extended = jnp.concatenate([rim_gated, gated], axis=0)
    conv_out = (
        conv_taps[0][None, :] * extended[:-2]
        + conv_taps[1][None, :] * extended[1:-1]
        + conv_taps[2][None, :] * extended[2:]
    )
    mixer_out = (bgate_float * conv_out).astype(BF16)
    weights = load_weights(core_arg, gate_weight[0], up_weight[0], down_weight[0])
    own, mixer_out, weights = lax.optimization_barrier((own, mixer_out, weights))
    gate_own, gate_peer, up_own, up_peer, down_own, down_peer = weights
    line = lax.axis_size("sp_0")
    spot = lax.axis_index("sp_0")
    token_half = tok_count // 2
    channels = mixer_out.shape[1]

    def half_of(array, which, dim):
        return lax.dynamic_slice_in_dim(array, which * token_half, token_half, dim)

    peer = swap(own)
    around = [mixer_out]
    for step in range(1, line):
        around.append(turned(mixer_out, "sp_0", step))
    parts = expert_own(own, gate_own, up_own, down_own)
    hidden, gate_pre, up_pre, part_theirs = expert_peer(
        peer, gate_peer, up_peer, down_peer, *parts
    )
    other = swap(part_theirs)
    part_mine = expert_mine(gate_pre, up_pre, gate_own, up_own)
    row_grads = add_parts(part_mine, other)
    row_grads, around = lax.optimization_barrier((row_grads, around))
    returned = exchange(row_grads.reshape(experts, capacity, width), SP).reshape(slots, width)
    grads_w = weight_grads(core_arg, own, peer, hidden, gate_pre, up_pre)
    around = jnp.stack(around)
    mixers = jnp.concatenate(
        [lax.dynamic_slice_in_dim(around, (spot - k) % line, 1, 0) for k in range(line)], axis=0
    )
    mixers_mine = half_of(mixers, core, 1).reshape(line * token_half, channels)
    mixers_theirs = half_of(mixers, 1 - core, 1).reshape(line * token_half, channels)
    returned, (gate_g, up_g, down_g), mixers_mine, mixers_theirs = lax.optimization_barrier(
        (returned, grads_w, mixers_mine, mixers_theirs)
    )

    normed_grad = dot_tn(selector, returned)
    stream_float = stream.astype(F32)
    cot_float = cotangent.astype(F32)
    inverse = lax.rsqrt(total[0] / D + EPSILON)[:, None]
    cross_part = jnp.sum(stream_float * gain_row * normed_grad, axis=1)
    cross = cross_part + swap(cross_part)
    stream_grad = (
        cot_float
        + inverse * gain_row * normed_grad
        - stream_float * inverse * inverse * inverse * cross[:, None] / D
    ).astype(BF16)

    grad_peer = swap(stream_grad)
    mine_half, peer_half = half_of(stream_grad, core, 0), half_of(grad_peer, core, 0)
    low = jnp.where(core == 0, mine_half, peer_half)
    high = jnp.where(core == 0, peer_half, mine_half)
    quarter = 2 * width // line
    parts = [low[:, :quarter], low[:, quarter:], high[:, :quarter], high[:, quarter:]]
    sent = jnp.stack(parts)
    grads_mine = exchange(sent, "sp_0").reshape(line * token_half, quarter)
    grads_theirs = swap(grads_mine)
    proj_part = dot_tn(grads_mine, mixers_mine) + dot_tn(grads_theirs, mixers_theirs)
    late_grad, late_peer, proj_part = lax.optimization_barrier((stream_grad, grad_peer, proj_part))
    plane = lax.axis_size(("sp_1", "sp_2"))
    arrived = exchange(proj_part.reshape(plane, quarter // plane, channels), ("sp_1", "sp_2"))
    proj_grad = arrived.sum(axis=0)

    proj_mine = lax.dynamic_slice_in_dim(out_proj, core * width, width, 0)
    proj_peer = lax.dynamic_slice_in_dim(out_proj, (1 - core) * width, width, 0)
    mixer_grad = dot_nn(late_grad, proj_mine) + dot_nn(late_peer, proj_peer)
    delta = mixer_grad * bgate_float
    next_rim = shifted(delta[:2], SP, -1)
    extended_back = jnp.concatenate([delta, next_rim], axis=0)
    gated_grad = (
        conv_taps[2][None, :] * extended_back[:-2]
        + conv_taps[1][None, :] * extended_back[1:-1]
        + conv_taps[0][None, :] * extended_back[2:]
    )
    bgate_grad = (mixer_grad * conv_out).astype(BF16)
    input_grad = (gated_grad * cgate_float).astype(BF16)
    cgate_grad = (gated_grad * input_float).astype(BF16)
    return (
        stream_grad,
        proj_grad,
        input_grad,
        bgate_grad,
        cgate_grad,
        gate_g[None],
        up_g[None],
        down_g[None],
    )


def solution(mesh):
    finer = Mesh(mesh.devices.reshape(4, 4, 4, mesh.shape["tp"]), ("sp_0", "sp_1", "sp_2", "tp"))
    return jax.shard_map(
        stage,
        mesh=finer,
        in_specs=(
            P(SP, "tp"),
            P("tp"),
            P(SP, "tp"),
            P(SP, None),
            P(SP, None),
            P(SP, "tp"),
            P(SP, "tp"),
            P(SP, "tp"),
            P(None, "tp"),
            P(None, "tp"),
            P(SP, None, "tp"),
            P(SP, None, "tp"),
            P(SP, "tp", None),
        ),
        out_specs=(
            P(SP, "tp"),
            P(SP, "tp"),
            P(SP, "tp"),
            P(SP, "tp"),
            P(SP, "tp"),
            P(SP, None, "tp"),
            P(SP, None, "tp"),
            P(SP, "tp", None),
        ),
        check_vma=False,
    )
```

```python
import jax
import jax.numpy as jnp
from jax import lax
from jax.experimental import pallas as pl
from jax.experimental.pallas import tpu as pltpu
from jax.sharding import Mesh
from jax.sharding import PartitionSpec as P


D = 2048
SP = ("sp_0", "sp_1", "sp_2")
EPSILON = 1e-06
VMEM = 56 * 1024 * 1024
EXPERT_BLOCKS = 2
F32 = jnp.float32
BF16 = jnp.bfloat16


def dot_nn(a, b):
    return lax.dot_general(a, b, (((1,), (0,)), ((), ())), preferred_element_type=F32)


def dot_nt(a, b):
    return lax.dot_general(a, b, (((1,), (1,)), ((), ())), preferred_element_type=F32)


def dot_tn(a, b):
    return lax.dot_general(a, b, (((0,), (0,)), ((), ())), preferred_element_type=F32)


def cost(flops, size):
    return pl.CostEstimate(flops=flops, transcendentals=0, bytes_accessed=size)


def swap(value):
    return lax.ppermute(value, "tp", [(0, 1), (1, 0)])


def exchange(value, axis):
    return lax.all_to_all(value, axis, split_axis=0, concat_axis=0, tiled=True)


def shifted(value, axis, steps):
    count = lax.axis_size(axis)
    leading, last = (max(0, -steps), min(count, count - steps))
    return lax.ppermute(value, axis, [(source, source + steps) for source in range(leading, last)])


def turned(value, axis, steps):
    count = lax.axis_size(axis)
    return lax.ppermute(value, axis, [(i, (i + steps) % count) for i in range(count)])


def slots_body(experts, capacity, stream_ref, routes_ref, squares_ref, target_ref):
    values = stream_ref[...].astype(F32)
    squares = values * values
    high = squares.astype(BF16)
    low = (squares - high.astype(F32)).astype(BF16)
    ones = jnp.ones((8, values.shape[1]), BF16)
    squares_ref[...] = (dot_nt(ones, high) + dot_nt(ones, low))[0:1]
    tokens = values.shape[0]
    first, second = routes_ref[0:1, :], routes_ref[1:2, :]
    ids = lax.broadcasted_iota(jnp.int32, (experts, tokens), 0)
    named_first = (ids == first).astype(F32)
    named_second = (ids == second).astype(F32)
    before = (
        lax.broadcasted_iota(jnp.int32, (tokens, tokens), 0)
        < lax.broadcasted_iota(jnp.int32, (tokens, tokens), 1)
    ).astype(F32)
    earlier = dot_nn((named_first + named_second).astype(BF16), before.astype(BF16))
    rank_first = jnp.sum(named_first * earlier, axis=0, keepdims=True).astype(jnp.int32)
    rank_second = jnp.sum(named_second * earlier, axis=0, keepdims=True).astype(jnp.int32)
    target_ref[0:1, :] = first * capacity + rank_first
    target_ref[1:2, :] = second * capacity + rank_second


def find_slots(stream, routes, experts, capacity):
    tokens = stream.shape[0]

    def body(*refs):
        slots_body(experts, capacity, *refs)

    return pl.pallas_call(
        body,
        out_shape=(
            jax.ShapeDtypeStruct((1, tokens), F32),
            jax.ShapeDtypeStruct((2, tokens), jnp.int32),
        ),
        name="find_slots",
        cost_estimate=cost(10**8, stream.size * 2),
    )(stream, routes)


def grads_body(target_ref, weight_ref, cot_ref, out_ref, sel_ref):
    rows, tokens = sel_ref.shape
    slots = lax.broadcasted_iota(jnp.int32, (rows, tokens), 0) + pl.program_id(0) * rows
    first = slots == target_ref[0:1, :]
    second = slots == target_ref[1:2, :]
    selector = jnp.where(first | second, 1.0, 0.0).astype(BF16)
    weight = jnp.where(first, weight_ref[0:1, :], 0.0) + jnp.where(second, weight_ref[1:2, :], 0.0)
    weight = jnp.sum(weight, axis=1, keepdims=True)
    sel_ref[...] = selector
    out_ref[...] = (weight * dot_nn(selector, cot_ref[...])).astype(BF16)


def inputs_body(own_ref, peer_ref, sel_ref, stream_ref, gain_ref, rows_ref, out_ref):
    inverse = lax.rsqrt((own_ref[...] + peer_ref[...]) / D + EPSILON)
    selector = sel_ref[...]
    scale = jnp.sum(selector.astype(F32) * inverse, axis=1, keepdims=True)
    inputs = dot_nn(selector, stream_ref[...])
    out_ref[...] = (inputs * scale * gain_ref[...]).astype(BF16)


def whole_block(*shape):
    return pl.BlockSpec(shape, lambda i: (0, 0))


def grad_rows(target, weights, cot, slots, steps):
    tokens, width = cot.shape
    rows = slots // steps
    return pl.pallas_call(
        grads_body,
        grid=(steps,),
        in_specs=[whole_block(2, tokens), whole_block(2, tokens), whole_block(tokens, width)],
        out_specs=(
            pl.BlockSpec((rows, width), lambda i: (i, 1)),
            pl.BlockSpec((rows, tokens), lambda i: (i, 0)),
        ),
        out_shape=(
            jax.ShapeDtypeStruct((slots, 2 * width), BF16),
            jax.ShapeDtypeStruct((slots, tokens), BF16),
        ),
        name="grad_rows",
        cost_estimate=cost(2 * slots * tokens * width, slots * width * 2),
    )(target, weights, cot)


def input_rows(own_squares, peer_squares, selector, stream, gain, rows_in, steps):
    tokens, width = stream.shape
    slots = selector.shape[0]
    rows = slots // steps
    return pl.pallas_call(
        inputs_body,
        grid=(steps,),
        in_specs=[
            whole_block(1, tokens),
            whole_block(1, tokens),
            pl.BlockSpec((rows, tokens), lambda i: (i, 0)),
            whole_block(tokens, width),
            whole_block(1, width),
            pl.BlockSpec(memory_space=pl.ANY),
        ],
        out_specs=pl.BlockSpec((rows, width), lambda i: (i, 0)),
        out_shape=jax.ShapeDtypeStruct((slots, 2 * width), BF16),
        input_output_aliases={5: 0},
        name="input_rows",
        cost_estimate=cost(2 * slots * tokens * width, slots * width * 2),
    )(own_squares, peer_squares, selector, stream, gain, rows_in)


def own_body(
    core_ref, own_hbm, gate_hbm, up_hbm, down_hbm,
    gate_out, up_out, grad_out, gate_own, up_own, gate_peer, up_peer, down_peer,
    own_ref, down_own, sems,
):
    _, step, double = own_ref.shape
    width = double // 2
    mine = pl.multiple_of(core_ref[0] * width, width)
    other = pl.multiple_of((1 - core_ref[0]) * width, width)
    moves = (
        (gate_hbm.at[pl.ds(mine, width), :], gate_own),
        (own_hbm.at[pl.ds(0, step), :], own_ref.at[0]),
        (up_hbm.at[pl.ds(mine, width), :], up_own),
        (down_hbm.at[:, pl.ds(mine, width)], down_own),
        (own_hbm.at[pl.ds(step, step), :], own_ref.at[1]),
        (gate_hbm.at[pl.ds(other, width), :], gate_peer),
        (up_hbm.at[pl.ds(other, width), :], up_peer),
        (down_hbm.at[:, pl.ds(other, width)], down_peer),
    )
    copies = [pltpu.make_async_copy(a, b, sems.at[i]) for i, (a, b) in enumerate(moves)]
    for copy in copies[:5]:
        copy.start()
    first, second = pl.ds(0, step), pl.ds(step, step)
    copies[0].wait()
    copies[1].wait()
    gate_out[first, :] = dot_nn(own_ref[0, :, :width], gate_own[...])
    for copy in copies[5:]:
        copy.start()
    copies[2].wait()
    up_out[first, :] = dot_nn(own_ref[0, :, :width], up_own[...])
    copies[3].wait()
    grad_out[first, :] = dot_nt(own_ref[0, :, width:], down_own[...])
    copies[4].wait()
    gate_out[second, :] = dot_nn(own_ref[1, :, :width], gate_own[...])
    up_out[second, :] = dot_nn(own_ref[1, :, :width], up_own[...])
    grad_out[second, :] = dot_nt(own_ref[1, :, width:], down_own[...])
    for copy in copies[5:]:
        copy.wait()


def peer_body(
    peer_ref, gate_w, up_w, down_w, gate_in, up_in, grad_in,
    hidden_ref, gate_ref, up_ref, theirs_ref,
):
    rows, double = peer_ref.shape
    width = double // 2
    step = rows // EXPERT_BLOCKS

    def block(i, carry):
        at = pl.ds(i * step, step)
        x, y = peer_ref[at, :width], peer_ref[at, width:]
        gate_lin = gate_in[at, :] + dot_nn(x, gate_w[...])
        up_lin = up_in[at, :] + dot_nn(x, up_w[...])
        hidden_grad = grad_in[at, :] + dot_nt(y, down_w[...])
        sig = jax.nn.sigmoid(gate_lin)
        silu = gate_lin * sig
        hidden_ref[at, :] = (silu * up_lin).astype(BF16)
        gate_pre = (hidden_grad * up_lin * sig * (1.0 + gate_lin * (1.0 - sig))).astype(BF16)
        up_pre = (hidden_grad * silu).astype(BF16)
        gate_ref[at, :] = gate_pre
        up_ref[at, :] = up_pre
        theirs_ref[at, :] = (dot_nt(gate_pre, gate_w[...]) + dot_nt(up_pre, up_w[...])).astype(BF16)
        return carry

    lax.fori_loop(0, EXPERT_BLOCKS, block, 0)


def mine_body(gate_ref, up_ref, gate_w, up_w, mine_ref):
    step = mine_ref.shape[0] // EXPERT_BLOCKS

    def block(i, carry):
        at = pl.ds(i * step, step)
        part = dot_nt(gate_ref[at, :], gate_w[...]) + dot_nt(up_ref[at, :], up_w[...])
        mine_ref[at, :] = part.astype(BF16)
        return carry

    lax.fori_loop(0, EXPERT_BLOCKS, block, 0)


def add_body(mine_ref, other_ref, out_ref, scratch, sems):
    blocks, step, _ = scratch.shape
    copies = []
    for i in range(blocks):
        at = pl.ds(i * step, step)
        total = mine_ref[at, :].astype(F32) + other_ref[at, :].astype(F32)
        scratch[i] = total.astype(BF16)
        copies.append(pltpu.make_async_copy(scratch.at[i], out_ref.at[at, :], sems.at[i]))
        copies[-1].start()
    for copy in copies:
        copy.wait()


IN_VMEM = pl.BlockSpec(memory_space=pltpu.VMEM)


def in_hbm(array):
    return pltpu.with_memory_space_constraint(array, pltpu.HBM)


def on_chip(body, outs, flops, limit, *args):
    return pl.pallas_call(
        body,
        in_specs=[IN_VMEM] * len(args),
        out_specs=[IN_VMEM] * len(outs),
        out_shape=[jax.ShapeDtypeStruct(s, d) for s, d in outs],
        compiler_params=pltpu.CompilerParams(vmem_limit_bytes=limit * 1024 * 1024),
        cost_estimate=cost(flops, 16 * 1024 * 1024),
    )(*args)


def expert_own(core, own, gate_w, up_w, down_w):
    rows, double = own.shape
    units = gate_w.shape[1]
    width = double // 2
    shapes = [((rows, units), F32)] * 3 + [((width, units), BF16)] * 4 + [((units, width), BF16)]
    return pl.pallas_call(
        own_body,
        in_specs=[pl.BlockSpec(memory_space=pltpu.SMEM)] + [pl.BlockSpec(memory_space=pl.ANY)] * 4,
        out_specs=[IN_VMEM] * len(shapes),
        out_shape=[jax.ShapeDtypeStruct(s, d) for s, d in shapes],
        scratch_shapes=[
            pltpu.VMEM((2, rows // 2, double), BF16),
            pltpu.VMEM((units, width), BF16),
            pltpu.SemaphoreType.DMA((8,)),
        ],
        compiler_params=pltpu.CompilerParams(vmem_limit_bytes=12 * 1024 * 1024),
        name="expert_own",
        cost_estimate=cost(3 * rows * double * units, 10 * double * units),
    )(core, *[in_hbm(array) for array in (own, gate_w, up_w, down_w)])


def expert_peer(peer, gate_w, up_w, down_w, *parts):
    rows, units = peer.shape[0], gate_w.shape[1]
    outs = [((rows, units), BF16)] * 3 + [((rows, peer.shape[1] // 2), BF16)]
    flops = 5 * rows * peer.shape[1] * units
    return on_chip(peer_body, outs, flops, 16, peer, gate_w, up_w, down_w, *parts)


def expert_mine(gate_pre, up_pre, gate_w, up_w):
    rows, width = gate_pre.shape[0], gate_w.shape[0]
    flops = 4 * rows * width * gate_w.shape[1]
    outs = [((rows, width), BF16)]
    return on_chip(mine_body, outs, flops, 8, gate_pre, up_pre, gate_w, up_w)[0]


def add_parts(mine, other):
    rows, width = mine.shape
    blocks = 8
    return pl.pallas_call(
        add_body,
        in_specs=[IN_VMEM] * 2,
        out_specs=pl.BlockSpec(memory_space=pltpu.HBM),
        out_shape=pltpu.HBM(mine.shape, BF16),
        scratch_shapes=[
            pltpu.VMEM((blocks, rows // blocks, width), BF16),
            pltpu.SemaphoreType.DMA((blocks,)),
        ],
        compiler_params=pltpu.CompilerParams(vmem_limit_bytes=8 * 1024 * 1024),
        name="add_parts",
        cost_estimate=cost(mine.size, 6 * mine.size),
    )(mine, other)


def product_body(left_ref, right_ref, out_ref):
    out_ref[...] = dot_tn(left_ref[...], right_ref[...])


def product_more_body(left_ref, right_ref, part_ref, out_ref):
    out_ref[...] = part_ref[...] + dot_tn(left_ref[...], right_ref[...])


def product(left, right, *part):
    body = product_more_body if part else product_body
    outs = [((left.shape[1], right.shape[1]), F32)]
    flops = 2 * left.size * right.shape[1]
    return on_chip(body, outs, flops, 8, left, right, *part)[0]


def mixer_body(core_ref, grad_ref, peer_ref, proj_ref, gate_ref, conv_ref, delta_ref, out_ref):
    width = grad_ref.shape[1]
    mine = pl.multiple_of(core_ref[0] * width, width)
    other = pl.multiple_of((1 - core_ref[0]) * width, width)
    mixer_grad = dot_nn(grad_ref[...], proj_ref[pl.ds(mine, width), :])
    mixer_grad = mixer_grad + dot_nn(peer_ref[...], proj_ref[pl.ds(other, width), :])
    delta_ref[...] = mixer_grad * gate_ref[...].astype(F32)
    out_ref[...] = (mixer_grad * conv_ref[...]).astype(BF16)


def mixer_back(core, grad, peer, proj, gate, conv):
    rows, width = grad.shape
    channels = proj.shape[1]
    return pl.pallas_call(
        mixer_body,
        in_specs=[pl.BlockSpec(memory_space=pltpu.SMEM)] + [IN_VMEM] * 5,
        out_specs=[IN_VMEM] * 2,
        out_shape=[
            jax.ShapeDtypeStruct((rows, channels), F32),
            jax.ShapeDtypeStruct((rows, channels), BF16),
        ],
        compiler_params=pltpu.CompilerParams(vmem_limit_bytes=12 * 1024 * 1024),
        name="mixer_back",
        cost_estimate=cost(4 * rows * width * channels, 8 * 1024 * 1024),
    )(core, grad, peer, proj, gate, conv)


def weights_body(
    core_ref, own_x, own_y, peer_x, peer_y, hidden_ref, gate_ref, up_ref,
    gate_out, up_out, down_out,
):
    def emit(x, y):
        gate_out[...] = dot_tn(x, gate_ref[...])
        up_out[...] = dot_tn(x, up_ref[...])
        down_out[...] = dot_tn(hidden_ref[...], y)

    half = pl.num_programs(0) // 2

    @pl.when(pl.program_id(0) < half)
    def _():
        emit(own_x[...], own_y[...])

    @pl.when(pl.program_id(0) >= half)
    def _():
        emit(peer_x[...], peer_y[...])


def weight_grads(core, own, peer, hidden, gate_pre, up_pre):
    rows, double = own.shape
    width = double // 2
    units = hidden.shape[1]
    chunk = 256
    half = width // chunk

    def own_at(base):
        return pl.BlockSpec((rows, chunk), lambda s, c: (0, base + jnp.minimum(s, half - 1)))

    def peer_at(base):
        return pl.BlockSpec((rows, chunk), lambda s, c: (0, base + jnp.maximum(s - half, 0)))

    def place(s, c):
        side = jnp.where(s < half, c[0], 1 - c[0])
        return side * half + jnp.where(s < half, s, s - half)

    whole = pl.BlockSpec((rows, units), lambda s, c: (0, 0))
    tall = pl.BlockSpec((chunk, units), lambda s, c: (place(s, c), 0))
    wide = pl.BlockSpec((units, chunk), lambda s, c: (0, place(s, c)))
    return pl.pallas_call(
        weights_body,
        grid_spec=pltpu.PrefetchScalarGridSpec(
            num_scalar_prefetch=1,
            grid=(2 * half,),
            in_specs=[own_at(0), own_at(half), peer_at(0), peer_at(half), whole, whole, whole],
            out_specs=[tall, tall, wide],
        ),
        out_shape=[
            jax.ShapeDtypeStruct((double, units), F32),
            jax.ShapeDtypeStruct((double, units), F32),
            jax.ShapeDtypeStruct((units, double), F32),
        ],
        compiler_params=pltpu.CompilerParams(vmem_limit_bytes=VMEM),
        name="weight_grads",
        cost_estimate=cost(12 * rows * width * units, 24 * width * units),
    )(core, own, own, peer, peer, hidden, gate_pre, up_pre)


def stage(
    stream,
    norm_gain,
    cotangent,
    route_weights,
    routes,
    conv_input,
    conv_bgate,
    conv_cgate,
    conv_taps,
    out_proj,
    gate_weight,
    up_weight,
    down_weight,
):
    experts = lax.axis_size(SP)
    tok_count, width = stream.shape
    top_count = routes.shape[1]
    capacity = 2 * tok_count * top_count // experts
    slots = experts * capacity
    core = lax.axis_index("tp")
    core_arg = core.astype(jnp.int32).reshape(1)
    gain_row = norm_gain[None, :]

    squares, target = find_slots(stream, routes.T, experts, capacity)
    peer_squares = swap(squares)
    rows, selector = grad_rows(target, route_weights.T, cotangent, slots, 4)
    rows = input_rows(squares, peer_squares, selector, stream, gain_row, rows, 4)
    own = exchange(rows.reshape(experts, capacity, 2 * width), SP).reshape(slots, 2 * width)

    input_float = conv_input.astype(F32)
    cgate_float = conv_cgate.astype(F32)
    bgate_float = conv_bgate.astype(F32)
    rim_rows = shifted(jnp.stack([conv_input[-2:], conv_cgate[-2:]]), SP, 1)
    rim_gated = rim_rows[1].astype(F32) * rim_rows[0].astype(F32)
    gated = cgate_float * input_float
    extended = jnp.concatenate([rim_gated, gated], axis=0)
    conv_out = (
        conv_taps[0][None, :] * extended[:-2]
        + conv_taps[1][None, :] * extended[1:-1]
        + conv_taps[2][None, :] * extended[2:]
    )
    mixer_out = (bgate_float * conv_out).astype(BF16)
    own, mixer_out = lax.optimization_barrier((own, mixer_out))
    line = lax.axis_size("sp_0")
    spot = lax.axis_index("sp_0")
    token_half = tok_count // 2
    channels = mixer_out.shape[1]

    def half_of(array, which, dim):
        return lax.dynamic_slice_in_dim(array, which * token_half, token_half, dim)

    peer = swap(own)
    around = [mixer_out]
    for step in range(1, line):
        around.append(turned(mixer_out, "sp_0", step))
    gate_part, up_part, grad_part, gate_own, up_own, gate_peer, up_peer, down_peer = expert_own(
        core_arg, own, gate_weight[0], up_weight[0], down_weight[0]
    )
    hidden, gate_pre, up_pre, part_theirs = expert_peer(
        peer, gate_peer, up_peer, down_peer, gate_part, up_part, grad_part
    )
    other = swap(part_theirs)
    part_mine = expert_mine(gate_pre, up_pre, gate_own, up_own)
    row_grads = add_parts(part_mine, other)
    returned = exchange(row_grads.reshape(experts, capacity, width), SP).reshape(slots, width)
    grads_w = weight_grads(core_arg, own, peer, hidden, gate_pre, up_pre)
    around = jnp.stack(around)
    mixers = jnp.concatenate(
        [lax.dynamic_slice_in_dim(around, (spot - k) % line, 1, 0) for k in range(line)], axis=0
    )
    mixers_mine = half_of(mixers, core, 1).reshape(line * token_half, channels)
    mixers_theirs = half_of(mixers, 1 - core, 1).reshape(line * token_half, channels)
    returned, (gate_g, up_g, down_g), mixers_mine, mixers_theirs = lax.optimization_barrier(
        (returned, grads_w, mixers_mine, mixers_theirs)
    )

    normed_grad = dot_tn(selector, returned)
    stream_float = stream.astype(F32)
    cot_float = cotangent.astype(F32)
    inverse = lax.rsqrt((squares + peer_squares)[0] / D + EPSILON)[:, None]
    cross_part = jnp.sum(stream_float * gain_row * normed_grad, axis=1)
    cross = cross_part + swap(cross_part)
    stream_grad = (
        cot_float
        + inverse * gain_row * normed_grad
        - stream_float * inverse * inverse * inverse * cross[:, None] / D
    ).astype(BF16)

    grad_peer = swap(stream_grad)
    mine_half, peer_half = half_of(stream_grad, core, 0), half_of(grad_peer, core, 0)
    low = jnp.where(core == 0, mine_half, peer_half)
    high = jnp.where(core == 0, peer_half, mine_half)
    quarter = 2 * width // line
    parts = [low[:, :quarter], low[:, quarter:], high[:, :quarter], high[:, quarter:]]
    sent = jnp.stack(parts)
    grads_mine = exchange(sent, "sp_0").reshape(line * token_half, quarter)
    grads_theirs = swap(grads_mine)
    proj_part = product(grads_theirs, mixers_theirs, product(grads_mine, mixers_mine))
    plane = lax.axis_size(("sp_1", "sp_2"))
    arrived = exchange(proj_part.reshape(plane, quarter // plane, channels), ("sp_1", "sp_2"))
    proj_grad = arrived.sum(axis=0)

    delta, bgate_grad = mixer_back(core_arg, stream_grad, grad_peer, out_proj, conv_bgate, conv_out)
    next_rim = shifted(delta[:2], SP, -1)
    extended_back = jnp.concatenate([delta, next_rim], axis=0)
    gated_grad = (
        conv_taps[2][None, :] * extended_back[:-2]
        + conv_taps[1][None, :] * extended_back[1:-1]
        + conv_taps[0][None, :] * extended_back[2:]
    )
    input_grad = (gated_grad * cgate_float).astype(BF16)
    cgate_grad = (gated_grad * input_float).astype(BF16)
    return (
        stream_grad,
        proj_grad,
        input_grad,
        bgate_grad,
        cgate_grad,
        gate_g[None],
        up_g[None],
        down_g[None],
    )


def solution(mesh):
    finer = Mesh(mesh.devices.reshape(4, 4, 4, mesh.shape["tp"]), ("sp_0", "sp_1", "sp_2", "tp"))
    return jax.shard_map(
        stage,
        mesh=finer,
        in_specs=(
            P(SP, "tp"),
            P("tp"),
            P(SP, "tp"),
            P(SP, None),
            P(SP, None),
            P(SP, "tp"),
            P(SP, "tp"),
            P(SP, "tp"),
            P(None, "tp"),
            P(None, "tp"),
            P(SP, None, "tp"),
            P(SP, None, "tp"),
            P(SP, "tp", None),
        ),
        out_specs=(
            P(SP, "tp"),
            P(SP, "tp"),
            P(SP, "tp"),
            P(SP, "tp"),
            P(SP, "tp"),
            P(SP, None, "tp"),
            P(SP, None, "tp"),
            P(SP, "tp", None),
        ),
        check_vma=False,
    )
```

```python
import jax
import jax.numpy as jnp
from jax import lax
from jax.experimental import pallas as pl
from jax.experimental.pallas import tpu as pltpu
from jax.sharding import Mesh
from jax.sharding import PartitionSpec as P


D = 2048
SP = ("sp_0", "sp_1", "sp_2")
EPSILON = 1e-06
VMEM = 56 * 1024 * 1024
F32 = jnp.float32
BF16 = jnp.bfloat16
IN_VMEM = pl.BlockSpec(memory_space=pltpu.VMEM)
IN_HBM = pl.BlockSpec(memory_space=pl.ANY)
IN_SMEM = pl.BlockSpec(memory_space=pltpu.SMEM)


def dot_nn(a, b):
    return lax.dot_general(a, b, (((1,), (0,)), ((), ())), preferred_element_type=F32)


def dot_nt(a, b):
    return lax.dot_general(a, b, (((1,), (1,)), ((), ())), preferred_element_type=F32)


def dot_tn(a, b):
    return lax.dot_general(a, b, (((0,), (0,)), ((), ())), preferred_element_type=F32)


def cost(flops, size):
    return pl.CostEstimate(flops=flops, transcendentals=0, bytes_accessed=size)


def swap(value):
    return lax.ppermute(value, "tp", [(0, 1), (1, 0)])


def exchange(value, axis):
    return lax.all_to_all(value, axis, split_axis=0, concat_axis=0, tiled=True)


def shifted(value, axis, steps):
    count = lax.axis_size(axis)
    leading, last = (max(0, -steps), min(count, count - steps))
    return lax.ppermute(value, axis, [(source, source + steps) for source in range(leading, last)])


def turned(value, axis, steps):
    count = lax.axis_size(axis)
    return lax.ppermute(value, axis, [(i, (i + steps) % count) for i in range(count)])


def slots_body(experts, capacity, stream_ref, routes_ref, squares_ref, target_ref):
    values = stream_ref[...].astype(F32)
    squares = values * values
    high = squares.astype(BF16)
    low = (squares - high.astype(F32)).astype(BF16)
    ones = jnp.ones((8, values.shape[1]), BF16)
    squares_ref[...] = (dot_nt(ones, high) + dot_nt(ones, low))[0:1]
    tokens = values.shape[0]
    first, second = routes_ref[0:1, :], routes_ref[1:2, :]
    ids = lax.broadcasted_iota(jnp.int32, (experts, tokens), 0)
    named_first = (ids == first).astype(F32)
    named_second = (ids == second).astype(F32)
    before = (
        lax.broadcasted_iota(jnp.int32, (tokens, tokens), 0)
        < lax.broadcasted_iota(jnp.int32, (tokens, tokens), 1)
    ).astype(F32)
    earlier = dot_nn((named_first + named_second).astype(BF16), before.astype(BF16))
    rank_first = jnp.sum(named_first * earlier, axis=0, keepdims=True).astype(jnp.int32)
    rank_second = jnp.sum(named_second * earlier, axis=0, keepdims=True).astype(jnp.int32)
    target_ref[0:1, :] = first * capacity + rank_first
    target_ref[1:2, :] = second * capacity + rank_second


def find_slots(stream, routes, experts, capacity):
    tokens = stream.shape[0]

    def body(*refs):
        slots_body(experts, capacity, *refs)

    return pl.pallas_call(
        body,
        out_shape=(
            jax.ShapeDtypeStruct((1, tokens), F32),
            jax.ShapeDtypeStruct((2, tokens), jnp.int32),
        ),
        name="find_slots",
        cost_estimate=cost(10**8, stream.size * 2),
    )(stream, routes)


def rows_body(
    target_ref, weight_ref, own_ref, peer_ref, stream_ref, cot_ref, gain_ref,
    out_ref, sel_ref, inverse_ref,
):
    rows, tokens = sel_ref.shape
    width = stream_ref.shape[1]
    slots = lax.broadcasted_iota(jnp.int32, (rows, tokens), 0) + pl.program_id(0) * rows
    first = slots == target_ref[0:1, :]
    second = slots == target_ref[1:2, :]
    inverse = lax.rsqrt((own_ref[...] + peer_ref[...]) / D + EPSILON)
    inverse_ref[...] = inverse
    both = jnp.where(first | second, 1.0, 0.0)
    selector = both.astype(BF16)
    scale = jnp.sum(both * inverse, axis=1, keepdims=True)
    weight = jnp.where(first, weight_ref[0:1, :], 0.0) + jnp.where(second, weight_ref[1:2, :], 0.0)
    weight = jnp.sum(weight, axis=1, keepdims=True)
    sel_ref[...] = selector
    inputs = dot_nn(selector, stream_ref[...])
    out_ref[:, :width] = (inputs * scale * gain_ref[...]).astype(BF16)
    grads = dot_nn(selector, cot_ref[...])
    out_ref[:, width:] = (weight * grads).astype(BF16)


def build_rows(target, weights, own_squares, peer_squares, stream, cot, gain, slots):
    tokens, width = stream.shape
    steps = 4
    rows = slots // steps

    def whole(*shape):
        return pl.BlockSpec(shape, lambda i: (0, 0))

    return pl.pallas_call(
        rows_body,
        grid=(steps,),
        in_specs=[
            IN_VMEM,
            IN_VMEM,
            IN_VMEM,
            IN_VMEM,
            whole(tokens, width),
            whole(tokens, width),
            whole(1, width),
        ],
        out_specs=(
            pl.BlockSpec((rows, 2 * width), lambda i: (i, 0)),
            pl.BlockSpec((rows, tokens), lambda i: (i, 0)),
            whole(1, tokens),
        ),
        out_shape=(
            jax.ShapeDtypeStruct((slots, 2 * width), BF16),
            jax.ShapeDtypeStruct((slots, tokens), BF16),
            jax.ShapeDtypeStruct((1, tokens), F32),
        ),
        name="build_rows",
        cost_estimate=cost(4 * slots * tokens * width, slots * width * 4),
    )(target, weights, own_squares, peer_squares, stream, cot, gain)


def own_body(
    core_ref, own_hbm, gate_hbm, up_hbm, down_hbm,
    gate_out, up_out, grad_out, gate_own, up_own, gate_peer, up_peer, down_peer,
    own_ref, down_own, sems,
):
    _, step, double = own_ref.shape
    width = double // 2
    mine = pl.multiple_of(core_ref[0] * width, width)
    other = pl.multiple_of((1 - core_ref[0]) * width, width)
    moves = (
        (gate_hbm.at[pl.ds(mine, width), :], gate_own),
        (own_hbm.at[pl.ds(0, step), :], own_ref.at[0]),
        (up_hbm.at[pl.ds(mine, width), :], up_own),
        (down_hbm.at[:, pl.ds(mine, width)], down_own),
        (own_hbm.at[pl.ds(step, step), :], own_ref.at[1]),
        (gate_hbm.at[pl.ds(other, width), :], gate_peer),
        (up_hbm.at[pl.ds(other, width), :], up_peer),
        (down_hbm.at[:, pl.ds(other, width)], down_peer),
    )
    copies = [pltpu.make_async_copy(a, b, sems.at[i]) for i, (a, b) in enumerate(moves)]
    for copy in copies[:5]:
        copy.start()
    first, second = pl.ds(0, step), pl.ds(step, step)
    copies[0].wait()
    copies[1].wait()
    gate_out[first, :] = dot_nn(own_ref[0, :, :width], gate_own[...])
    for copy in copies[5:]:
        copy.start()
    copies[2].wait()
    up_out[first, :] = dot_nn(own_ref[0, :, :width], up_own[...])
    copies[3].wait()
    grad_out[first, :] = dot_nt(own_ref[0, :, width:], down_own[...])
    copies[4].wait()
    gate_out[second, :] = dot_nn(own_ref[1, :, :width], gate_own[...])
    up_out[second, :] = dot_nn(own_ref[1, :, :width], up_own[...])
    grad_out[second, :] = dot_nt(own_ref[1, :, width:], down_own[...])
    for copy in copies[5:]:
        copy.wait()


def peer_body(
    start, peer_hbm, gate_w, up_w, down_w, gate_in, up_in, grad_in,
    hidden_hbm, gate_ref, up_ref, theirs_ref, peer_ref, hidden_ref, sems,
):
    rows, double = peer_ref.shape
    width = double // 2
    half = rows // 2
    copies = []
    for i in range(2):
        source = peer_hbm.at[pl.ds(start + i * half, half), :]
        copies.append(
            pltpu.make_async_copy(source, peer_ref.at[pl.ds(i * half, half), :], sems.at[i])
        )
        copies[i].start()
    for copy in copies:
        copy.wait()
    at = pl.ds(start, rows)
    x, y = peer_ref[:, :width], peer_ref[:, width:]
    gate_lin = gate_in[at, :] + dot_nn(x, gate_w[...])
    up_lin = up_in[at, :] + dot_nn(x, up_w[...])
    hidden_grad = grad_in[at, :] + dot_nt(y, down_w[...])
    sig = jax.nn.sigmoid(gate_lin)
    silu = gate_lin * sig
    hidden_ref[...] = (silu * up_lin).astype(BF16)
    keep = pltpu.make_async_copy(hidden_ref, hidden_hbm, sems.at[2])
    keep.start()
    gate_pre = (hidden_grad * up_lin * sig * (1.0 + gate_lin * (1.0 - sig))).astype(BF16)
    up_pre = (hidden_grad * silu).astype(BF16)
    gate_ref[...] = gate_pre
    up_ref[...] = up_pre
    theirs_ref[...] = (dot_nt(gate_pre, gate_w[...]) + dot_nt(up_pre, up_w[...])).astype(BF16)
    keep.wait()


def mine_body(gate_a, gate_b, up_a, up_b, gate_w, up_w, mine_ref):
    half = mine_ref.shape[0] // 2
    for i, (gate_ref, up_ref) in enumerate(((gate_a, up_a), (gate_b, up_b))):
        part = dot_nt(gate_ref[...], gate_w[...]) + dot_nt(up_ref[...], up_w[...])
        mine_ref[pl.ds(i * half, half), :] = part.astype(BF16)


def add_body(mine_ref, other_a, other_b, out_ref, scratch, sems):
    blocks, step, _ = scratch.shape
    copies = []
    for i in range(blocks):
        at = pl.ds(i * step, step)
        other = (other_a, other_b)[2 * i // blocks]
        from_other = pl.ds(i % (blocks // 2) * step, step)
        total = mine_ref[at, :].astype(F32) + other[from_other, :].astype(F32)
        scratch[i] = total.astype(BF16)
        copies.append(pltpu.make_async_copy(scratch.at[i], out_ref.at[at, :], sems.at[i]))
        copies[-1].start()
    for copy in copies:
        copy.wait()


def in_hbm(array):
    return pltpu.with_memory_space_constraint(array, pltpu.HBM)


def on_chip(body, outs, flops, limit, *args):
    return pl.pallas_call(
        body,
        in_specs=[IN_VMEM] * len(args),
        out_specs=[IN_VMEM] * len(outs),
        out_shape=[jax.ShapeDtypeStruct(s, d) for s, d in outs],
        compiler_params=pltpu.CompilerParams(vmem_limit_bytes=limit * 1024 * 1024),
        cost_estimate=cost(flops, 16 * 1024 * 1024),
    )(*args)


def expert_own(core, own, gate_w, up_w, down_w):
    rows, double = own.shape
    units = gate_w.shape[1]
    width = double // 2
    shapes = [((rows, units), F32)] * 3 + [((width, units), BF16)] * 4 + [((units, width), BF16)]
    return pl.pallas_call(
        own_body,
        in_specs=[IN_SMEM] + [IN_HBM] * 4,
        out_specs=[IN_VMEM] * len(shapes),
        out_shape=[jax.ShapeDtypeStruct(s, d) for s, d in shapes],
        scratch_shapes=[
            pltpu.VMEM((2, rows // 2, double), BF16),
            pltpu.VMEM((units, width), BF16),
            pltpu.SemaphoreType.DMA((8,)),
        ],
        compiler_params=pltpu.CompilerParams(vmem_limit_bytes=12 * 1024 * 1024),
        name="expert_own",
        cost_estimate=cost(3 * rows * double * units, 10 * double * units),
    )(core, *[in_hbm(array) for array in (own, gate_w, up_w, down_w)])


def expert_peer(start, peer, gate_w, up_w, down_w, *parts):
    rows, double = peer.shape[0] // 2, peer.shape[1]
    units = gate_w.shape[1]
    outs = [((rows, units), BF16)] * 2 + [((rows, double // 2), BF16)]

    def body(*refs):
        peer_body(start, *refs)

    return pl.pallas_call(
        body,
        in_specs=[IN_HBM] + [IN_VMEM] * 6,
        out_specs=[IN_HBM] + [IN_VMEM] * len(outs),
        out_shape=[pltpu.HBM((rows, units), BF16)] + [jax.ShapeDtypeStruct(s, d) for s, d in outs],
        scratch_shapes=[
            pltpu.VMEM((rows, double), BF16),
            pltpu.VMEM((rows, units), BF16),
            pltpu.SemaphoreType.DMA((3,)),
        ],
        compiler_params=pltpu.CompilerParams(vmem_limit_bytes=16 * 1024 * 1024),
        name="expert_peer",
        cost_estimate=cost(5 * rows * double * units, 8 * rows * double),
    )(in_hbm(peer), gate_w, up_w, down_w, *parts)


def expert_mine(gate_a, gate_b, up_a, up_b, gate_w, up_w):
    rows, width = 2 * gate_a.shape[0], gate_w.shape[0]
    flops = 4 * rows * width * gate_w.shape[1]
    outs = [((rows, width), BF16)]
    return on_chip(mine_body, outs, flops, 8, gate_a, gate_b, up_a, up_b, gate_w, up_w)[0]


def add_parts(mine, other_a, other_b):
    rows, width = mine.shape
    blocks = 8
    return pl.pallas_call(
        add_body,
        in_specs=[IN_VMEM] * 3,
        out_specs=pl.BlockSpec(memory_space=pltpu.HBM),
        out_shape=pltpu.HBM(mine.shape, BF16),
        scratch_shapes=[
            pltpu.VMEM((blocks, rows // blocks, width), BF16),
            pltpu.SemaphoreType.DMA((blocks,)),
        ],
        compiler_params=pltpu.CompilerParams(vmem_limit_bytes=8 * 1024 * 1024),
        name="add_parts",
        cost_estimate=cost(mine.size, 6 * mine.size),
    )(mine, other_a, other_b)


def tick_body(in_ref, out_ref):
    out_ref[...] = in_ref[...]


def tick(array):
    return pl.pallas_call(
        tick_body, out_shape=jax.ShapeDtypeStruct(array.shape, array.dtype), name="tick"
    )(array)


def product_body(left_ref, right_ref, out_ref):
    out_ref[...] = dot_tn(left_ref[...], right_ref[...])


def product_more_body(left_ref, right_ref, part_ref, out_ref):
    out_ref[...] = part_ref[...] + dot_tn(left_ref[...], right_ref[...])


def product(left, right, *part):
    body = product_more_body if part else product_body
    outs = [((left.shape[1], right.shape[1]), F32)]
    flops = 2 * left.size * right.shape[1]
    return on_chip(body, outs, flops, 8, left, right, *part)[0]


def mixer_body(
    core_ref, grad_hbm, peer_hbm, proj_hbm, gate_ref, conv_ref, delta_ref, out_ref,
    grad_ref, peer_ref, proj_ref, sems,
):
    width = grad_ref.shape[1]
    mine = pl.multiple_of(core_ref[0] * width, width)
    other = pl.multiple_of((1 - core_ref[0]) * width, width)
    moves = (
        (proj_hbm.at[pl.ds(mine, width), :], proj_ref.at[0]),
        (grad_hbm, grad_ref),
        (proj_hbm.at[pl.ds(other, width), :], proj_ref.at[1]),
        (peer_hbm, peer_ref),
    )
    copies = [pltpu.make_async_copy(a, b, sems.at[i]) for i, (a, b) in enumerate(moves)]
    for copy in copies:
        copy.start()
    copies[0].wait()
    copies[1].wait()
    mixer_grad = dot_nn(grad_ref[...], proj_ref[0])
    copies[2].wait()
    copies[3].wait()
    mixer_grad = mixer_grad + dot_nn(peer_ref[...], proj_ref[1])
    delta_ref[...] = mixer_grad * gate_ref[...].astype(F32)
    out_ref[...] = (mixer_grad * conv_ref[...]).astype(BF16)


def mixer_back(core, grad, peer, proj, gate, conv):
    rows, width = grad.shape
    channels = proj.shape[1]
    return pl.pallas_call(
        mixer_body,
        in_specs=[IN_SMEM] + [IN_HBM] * 3 + [IN_VMEM] * 2,
        out_specs=[IN_VMEM] * 2,
        out_shape=[
            jax.ShapeDtypeStruct((rows, channels), F32),
            jax.ShapeDtypeStruct((rows, channels), BF16),
        ],
        scratch_shapes=[
            pltpu.VMEM((rows, width), BF16),
            pltpu.VMEM((rows, width), BF16),
            pltpu.VMEM((2, width, channels), BF16),
            pltpu.SemaphoreType.DMA((4,)),
        ],
        compiler_params=pltpu.CompilerParams(vmem_limit_bytes=12 * 1024 * 1024),
        name="mixer_back",
        cost_estimate=cost(4 * rows * width * channels, 8 * 1024 * 1024),
    )(core, in_hbm(grad), in_hbm(peer), in_hbm(proj), gate, conv)


def weights_body(
    core_ref, own_x, own_y, peer_x, peer_y, hidden_a, hidden_b, gate_a, gate_b, up_a, up_b,
    gate_out, up_out, down_out,
):
    half = hidden_a.shape[0]

    def emit(x_ref, y_ref):
        x_a, x_b = x_ref[:half, :], x_ref[half:, :]
        gate_out[...] = dot_tn(x_a, gate_a[...]) + dot_tn(x_b, gate_b[...])
        up_out[...] = dot_tn(x_a, up_a[...]) + dot_tn(x_b, up_b[...])
        down_out[...] = dot_tn(hidden_a[...], y_ref[:half, :]) + dot_tn(
            hidden_b[...], y_ref[half:, :]
        )

    steps = pl.num_programs(0) // 2

    @pl.when(pl.program_id(0) < steps)
    def _():
        emit(own_x, own_y)

    @pl.when(pl.program_id(0) >= steps)
    def _():
        emit(peer_x, peer_y)


def weight_grads(core, own, peer, *halves):
    rows, double = own.shape
    width = double // 2
    units = halves[0].shape[1]
    chunk = 256
    half = width // chunk

    def own_at(base):
        return pl.BlockSpec((rows, chunk), lambda s, c: (0, base + jnp.minimum(s, half - 1)))

    def peer_at(base):
        return pl.BlockSpec((rows, chunk), lambda s, c: (0, base + jnp.maximum(s - half, 0)))

    def place(s, c):
        side = jnp.where(s < half, c[0], 1 - c[0])
        return side * half + jnp.where(s < half, s, s - half)

    whole = pl.BlockSpec((rows // 2, units), lambda s, c: (0, 0))
    tall = pl.BlockSpec((chunk, units), lambda s, c: (place(s, c), 0))
    wide = pl.BlockSpec((units, chunk), lambda s, c: (0, place(s, c)))
    return pl.pallas_call(
        weights_body,
        grid_spec=pltpu.PrefetchScalarGridSpec(
            num_scalar_prefetch=1,
            grid=(2 * half,),
            in_specs=[own_at(0), own_at(half), peer_at(0), peer_at(half)] + [whole] * 6,
            out_specs=[tall, tall, wide],
        ),
        out_shape=[
            jax.ShapeDtypeStruct((double, units), F32),
            jax.ShapeDtypeStruct((double, units), F32),
            jax.ShapeDtypeStruct((units, double), F32),
        ],
        compiler_params=pltpu.CompilerParams(vmem_limit_bytes=VMEM),
        name="weight_grads",
        cost_estimate=cost(12 * rows * width * units, 24 * width * units),
    )(core, own, own, peer, peer, *halves)


def stage(
    stream,
    norm_gain,
    cotangent,
    route_weights,
    routes,
    conv_input,
    conv_bgate,
    conv_cgate,
    conv_taps,
    out_proj,
    gate_weight,
    up_weight,
    down_weight,
):
    experts = lax.axis_size(SP)
    tok_count, width = stream.shape
    top_count = routes.shape[1]
    capacity = 2 * tok_count * top_count // experts
    slots = experts * capacity
    core = lax.axis_index("tp")
    core_arg = core.astype(jnp.int32).reshape(1)
    gain_row = norm_gain[None, :]

    squares, target = find_slots(stream, routes.T, experts, capacity)
    peer_squares = swap(squares)
    rows, selector, inverse_row = build_rows(
        target, route_weights.T, squares, peer_squares, stream, cotangent, gain_row, slots
    )
    own = exchange(rows.reshape(experts, capacity, 2 * width), SP)
    own = own.reshape(slots, 2 * width)

    input_float = conv_input.astype(F32)
    cgate_float = conv_cgate.astype(F32)
    bgate_float = conv_bgate.astype(F32)
    rim_rows = shifted(jnp.stack([conv_input[-2:], conv_cgate[-2:]]), SP, 1)
    rim_gated = rim_rows[1].astype(F32) * rim_rows[0].astype(F32)
    gated = cgate_float * input_float
    extended = jnp.concatenate([rim_gated, gated], axis=0)
    conv_out = (
        conv_taps[0][None, :] * extended[:-2]
        + conv_taps[1][None, :] * extended[1:-1]
        + conv_taps[2][None, :] * extended[2:]
    )
    mixer_out = (bgate_float * conv_out).astype(BF16)
    line = lax.axis_size("sp_0")
    spot = lax.axis_index("sp_0")
    token_half = tok_count // 2
    channels = mixer_out.shape[1]

    def half_of(array, which, dim):
        return lax.dynamic_slice_in_dim(array, which * token_half, token_half, dim)

    inverse_row = tick(inverse_row)
    peer = swap(own)
    around = [mixer_out]
    for step in range(1, line):
        around.append(turned(mixer_out, "sp_0", step))
    gate_part, up_part, grad_part, gate_own, up_own, gate_peer, up_peer, down_peer = expert_own(
        core_arg, own, gate_weight[0], up_weight[0], down_weight[0]
    )
    more = (gate_peer, up_peer, down_peer, gate_part, up_part, grad_part)
    hidden_a, gate_a, up_a, theirs_a = expert_peer(0, peer, *more)
    other_a = swap(theirs_a)
    hidden_b, gate_b, up_b, theirs_b = expert_peer(slots // 2, peer, *more)
    other_b = swap(theirs_b)
    part_mine = expert_mine(gate_a, gate_b, up_a, up_b, gate_own, up_own)
    row_grads = add_parts(part_mine, other_a, other_b)
    returned = exchange(row_grads.reshape(experts, capacity, width), SP).reshape(slots, width)
    halves = (hidden_a, hidden_b, gate_a, gate_b, up_a, up_b)
    grads_w = weight_grads(core_arg, own, peer, *halves)
    around = jnp.stack(around)
    mixers = jnp.concatenate(
        [lax.dynamic_slice_in_dim(around, (spot - k) % line, 1, 0) for k in range(line)], axis=0
    )
    mixers_mine = half_of(mixers, core, 1).reshape(line * token_half, channels)
    mixers_theirs = half_of(mixers, 1 - core, 1).reshape(line * token_half, channels)
    returned, (gate_g, up_g, down_g), mixers_mine, mixers_theirs = lax.optimization_barrier(
        (returned, grads_w, mixers_mine, mixers_theirs)
    )

    normed_grad = dot_tn(selector, returned)
    stream_float = stream.astype(F32)
    cot_float = cotangent.astype(F32)
    inverse = inverse_row[0][:, None]
    cross_part = jnp.sum(stream_float * gain_row * normed_grad, axis=1)
    cross = cross_part + swap(cross_part)
    stream_grad = (
        cot_float
        + inverse * gain_row * normed_grad
        - stream_float * inverse * inverse * inverse * cross[:, None] / D
    ).astype(BF16)

    grad_peer = swap(stream_grad)
    mine_half, peer_half = half_of(stream_grad, core, 0), half_of(grad_peer, core, 0)
    low = jnp.where(core == 0, mine_half, peer_half)
    high = jnp.where(core == 0, peer_half, mine_half)
    quarter = 2 * width // line
    parts = [low[:, :quarter], low[:, quarter:], high[:, :quarter], high[:, quarter:]]
    sent = jnp.stack(parts)
    grads_mine = exchange(sent, "sp_0").reshape(line * token_half, quarter)
    delta, bgate_grad = mixer_back(core_arg, stream_grad, grad_peer, out_proj, conv_bgate, conv_out)
    next_rim = shifted(delta[:2], SP, -1)
    last_rows = tick(delta[-8:])
    grads_theirs = swap(grads_mine)
    proj_part = product(grads_theirs, mixers_theirs, product(grads_mine, mixers_mine))
    plane = lax.axis_size(("sp_1", "sp_2"))
    arrived = exchange(proj_part.reshape(plane, quarter // plane, channels), ("sp_1", "sp_2"))
    proj_grad = arrived.sum(axis=0)

    extended_back = jnp.concatenate([delta[:-8], last_rows, next_rim], axis=0)
    gated_grad = (
        conv_taps[2][None, :] * extended_back[:-2]
        + conv_taps[1][None, :] * extended_back[1:-1]
        + conv_taps[0][None, :] * extended_back[2:]
    )
    input_grad = (gated_grad * cgate_float).astype(BF16)
    cgate_grad = (gated_grad * input_float).astype(BF16)
    return (
        stream_grad,
        proj_grad,
        input_grad,
        bgate_grad,
        cgate_grad,
        gate_g[None],
        up_g[None],
        down_g[None],
    )


def solution(mesh):
    finer = Mesh(mesh.devices.reshape(4, 4, 4, mesh.shape["tp"]), ("sp_0", "sp_1", "sp_2", "tp"))
    return jax.shard_map(
        stage,
        mesh=finer,
        in_specs=(
            P(SP, "tp"),
            P("tp"),
            P(SP, "tp"),
            P(SP, None),
            P(SP, None),
            P(SP, "tp"),
            P(SP, "tp"),
            P(SP, "tp"),
            P(None, "tp"),
            P(None, "tp"),
            P(SP, None, "tp"),
            P(SP, None, "tp"),
            P(SP, "tp", None),
        ),
        out_specs=(
            P(SP, "tp"),
            P(SP, "tp"),
            P(SP, "tp"),
            P(SP, "tp"),
            P(SP, "tp"),
            P(SP, None, "tp"),
            P(SP, None, "tp"),
            P(SP, "tp", None),
        ),
        check_vma=False,
    )
```

```python
import jax
import jax.numpy as jnp
from jax import lax
from jax.experimental import pallas as pl
from jax.experimental.pallas import tpu as pltpu
from jax.sharding import Mesh
from jax.sharding import PartitionSpec as P


D = 2048
SP = ("sp_0", "sp_1", "sp_2")
EPSILON = 1e-06
VMEM = 56 * 1024 * 1024
F32 = jnp.float32
BF16 = jnp.bfloat16
IN_VMEM = pl.BlockSpec(memory_space=pltpu.VMEM)
IN_HBM = pl.BlockSpec(memory_space=pl.ANY)
IN_SMEM = pl.BlockSpec(memory_space=pltpu.SMEM)


def dot_nn(a, b):
    return lax.dot_general(a, b, (((1,), (0,)), ((), ())), preferred_element_type=F32)


def dot_nt(a, b):
    return lax.dot_general(a, b, (((1,), (1,)), ((), ())), preferred_element_type=F32)


def dot_tn(a, b):
    return lax.dot_general(a, b, (((0,), (0,)), ((), ())), preferred_element_type=F32)


def cost(flops, size):
    return pl.CostEstimate(flops=flops, transcendentals=0, bytes_accessed=size)


def swap(value):
    return lax.ppermute(value, "tp", [(0, 1), (1, 0)])


def exchange(value, axis):
    return lax.all_to_all(value, axis, split_axis=0, concat_axis=0, tiled=True)


def shifted(value, axis, steps):
    count = lax.axis_size(axis)
    leading, last = (max(0, -steps), min(count, count - steps))
    return lax.ppermute(value, axis, [(source, source + steps) for source in range(leading, last)])


def turned(value, axis, steps):
    count = lax.axis_size(axis)
    return lax.ppermute(value, axis, [(i, (i + steps) % count) for i in range(count)])


def slots_body(experts, capacity, stream_ref, routes_ref, squares_ref, target_ref):
    values = stream_ref[...].astype(F32)
    squares = values * values
    high = squares.astype(BF16)
    low = (squares - high.astype(F32)).astype(BF16)
    ones = jnp.ones((8, values.shape[1]), BF16)
    squares_ref[...] = (dot_nt(ones, high) + dot_nt(ones, low))[0:1]
    tokens = values.shape[0]
    first, second = routes_ref[0:1, :], routes_ref[1:2, :]
    ids = lax.broadcasted_iota(jnp.int32, (experts, tokens), 0)
    named_first = (ids == first).astype(F32)
    named_second = (ids == second).astype(F32)
    before = (
        lax.broadcasted_iota(jnp.int32, (tokens, tokens), 0)
        < lax.broadcasted_iota(jnp.int32, (tokens, tokens), 1)
    ).astype(F32)
    earlier = dot_nn((named_first + named_second).astype(BF16), before.astype(BF16))
    rank_first = jnp.sum(named_first * earlier, axis=0, keepdims=True).astype(jnp.int32)
    rank_second = jnp.sum(named_second * earlier, axis=0, keepdims=True).astype(jnp.int32)
    target_ref[0:1, :] = first * capacity + rank_first
    target_ref[1:2, :] = second * capacity + rank_second


def find_slots(stream, routes, experts, capacity):
    tokens = stream.shape[0]

    def body(*refs):
        slots_body(experts, capacity, *refs)

    return pl.pallas_call(
        body,
        out_shape=(
            jax.ShapeDtypeStruct((1, tokens), F32),
            jax.ShapeDtypeStruct((2, tokens), jnp.int32),
        ),
        name="find_slots",
        cost_estimate=cost(10**8, stream.size * 2),
    )(stream, routes)


def rows_body(
    target_ref, weight_ref, own_ref, peer_ref, stream_ref, cot_ref, gain_ref,
    out_ref, sel_ref, inverse_ref,
):
    rows, tokens = sel_ref.shape
    width = stream_ref.shape[1]
    slots = lax.broadcasted_iota(jnp.int32, (rows, tokens), 0) + pl.program_id(0) * rows
    first = slots == target_ref[0:1, :]
    second = slots == target_ref[1:2, :]
    inverse = lax.rsqrt((own_ref[...] + peer_ref[...]) / D + EPSILON)
    inverse_ref[...] = inverse
    both = jnp.where(first | second, 1.0, 0.0)
    selector = both.astype(BF16)
    scale = jnp.sum(both * inverse, axis=1, keepdims=True)
    weight = jnp.where(first, weight_ref[0:1, :], 0.0) + jnp.where(second, weight_ref[1:2, :], 0.0)
    weight = jnp.sum(weight, axis=1, keepdims=True)
    sel_ref[...] = selector
    inputs = dot_nn(selector, stream_ref[...])
    out_ref[:, :width] = (inputs * scale * gain_ref[...]).astype(BF16)
    grads = dot_nn(selector, cot_ref[...])
    out_ref[:, width:] = (weight * grads).astype(BF16)


def build_rows(target, weights, own_squares, peer_squares, stream, cot, gain, slots):
    tokens, width = stream.shape
    steps = 2
    rows = slots // steps

    def whole(*shape):
        return pl.BlockSpec(shape, lambda i: (0, 0))

    return pl.pallas_call(
        rows_body,
        grid=(steps,),
        in_specs=[
            IN_VMEM,
            IN_VMEM,
            IN_VMEM,
            IN_VMEM,
            whole(tokens, width),
            whole(tokens, width),
            whole(1, width),
        ],
        out_specs=(
            pl.BlockSpec((rows, 2 * width), lambda i: (i, 0)),
            pl.BlockSpec((rows, tokens), lambda i: (i, 0)),
            whole(1, tokens),
        ),
        out_shape=(
            jax.ShapeDtypeStruct((slots, 2 * width), BF16),
            jax.ShapeDtypeStruct((slots, tokens), BF16),
            jax.ShapeDtypeStruct((1, tokens), F32),
        ),
        name="build_rows",
        cost_estimate=cost(4 * slots * tokens * width, slots * width * 4),
    )(target, weights, own_squares, peer_squares, stream, cot, gain)


def own_body(
    core_ref, own_hbm, gate_hbm, up_hbm, down_hbm,
    gate_out, up_out, grad_out, gate_own, up_own, gate_peer, up_peer, down_peer,
    own_ref, down_own, sems,
):
    _, step, double = own_ref.shape
    width = double // 2
    mine = pl.multiple_of(core_ref[0] * width, width)
    other = pl.multiple_of((1 - core_ref[0]) * width, width)
    moves = (
        (gate_hbm.at[pl.ds(mine, width), :], gate_own),
        (own_hbm.at[pl.ds(0, step), :], own_ref.at[0]),
        (up_hbm.at[pl.ds(mine, width), :], up_own),
        (down_hbm.at[:, pl.ds(mine, width)], down_own),
        (own_hbm.at[pl.ds(step, step), :], own_ref.at[1]),
        (gate_hbm.at[pl.ds(other, width), :], gate_peer),
        (up_hbm.at[pl.ds(other, width), :], up_peer),
        (down_hbm.at[:, pl.ds(other, width)], down_peer),
    )
    copies = [pltpu.make_async_copy(a, b, sems.at[i]) for i, (a, b) in enumerate(moves)]
    for copy in copies[:5]:
        copy.start()
    first, second = pl.ds(0, step), pl.ds(step, step)
    copies[0].wait()
    copies[1].wait()
    gate_out[first, :] = dot_nn(own_ref[0, :, :width], gate_own[...])
    for copy in copies[5:]:
        copy.start()
    copies[2].wait()
    up_out[first, :] = dot_nn(own_ref[0, :, :width], up_own[...])
    copies[3].wait()
    grad_out[first, :] = dot_nt(own_ref[0, :, width:], down_own[...])
    copies[4].wait()
    gate_out[second, :] = dot_nn(own_ref[1, :, :width], gate_own[...])
    up_out[second, :] = dot_nn(own_ref[1, :, :width], up_own[...])
    grad_out[second, :] = dot_nt(own_ref[1, :, width:], down_own[...])
    for copy in copies[5:]:
        copy.wait()


def peer_body(
    start, peer_hbm, gate_w, up_w, down_w, gate_in, up_in, grad_in,
    hidden_hbm, gate_ref, up_ref, theirs_ref, peer_ref, hidden_ref, sems,
):
    rows, double = peer_ref.shape
    width = double // 2
    at = pl.ds(start, rows)
    copies = []
    for i in range(2):
        part = pl.ds(i * width, width)
        copies.append(
            pltpu.make_async_copy(peer_hbm.at[at, part], peer_ref.at[:, part], sems.at[i])
        )
        copies[i].start()
    copies[0].wait()
    x = peer_ref[:, :width]
    gate_lin = gate_in[at, :] + dot_nn(x, gate_w[...])
    up_lin = up_in[at, :] + dot_nn(x, up_w[...])
    copies[1].wait()
    y = peer_ref[:, width:]
    hidden_grad = grad_in[at, :] + dot_nt(y, down_w[...])
    sig = jax.nn.sigmoid(gate_lin)
    silu = gate_lin * sig
    hidden_ref[...] = (silu * up_lin).astype(BF16)
    keep = pltpu.make_async_copy(hidden_ref, hidden_hbm, sems.at[2])
    keep.start()
    gate_pre = (hidden_grad * up_lin * sig * (1.0 + gate_lin * (1.0 - sig))).astype(BF16)
    up_pre = (hidden_grad * silu).astype(BF16)
    gate_ref[...] = gate_pre
    up_ref[...] = up_pre
    theirs_ref[...] = (dot_nt(gate_pre, gate_w[...]) + dot_nt(up_pre, up_w[...])).astype(BF16)
    keep.wait()


def mine_body(gate_a, gate_b, up_a, up_b, gate_w, up_w, mine_ref):
    half = mine_ref.shape[0] // 2
    for i, (gate_ref, up_ref) in enumerate(((gate_a, up_a), (gate_b, up_b))):
        part = dot_nt(gate_ref[...], gate_w[...]) + dot_nt(up_ref[...], up_w[...])
        mine_ref[pl.ds(i * half, half), :] = part.astype(BF16)


def add_body(mine_ref, other_a, other_b, out_ref, scratch, sems):
    blocks, step, _ = scratch.shape
    copies = []
    for i in range(blocks):
        at = pl.ds(i * step, step)
        other = (other_a, other_b)[2 * i // blocks]
        from_other = pl.ds(i % (blocks // 2) * step, step)
        total = mine_ref[at, :].astype(F32) + other[from_other, :].astype(F32)
        scratch[i] = total.astype(BF16)
        copies.append(pltpu.make_async_copy(scratch.at[i], out_ref.at[at, :], sems.at[i]))
        copies[-1].start()
    for copy in copies:
        copy.wait()


def in_hbm(array):
    return pltpu.with_memory_space_constraint(array, pltpu.HBM)


def on_chip(body, outs, flops, limit, *args):
    return pl.pallas_call(
        body,
        in_specs=[IN_VMEM] * len(args),
        out_specs=[IN_VMEM] * len(outs),
        out_shape=[jax.ShapeDtypeStruct(s, d) for s, d in outs],
        compiler_params=pltpu.CompilerParams(vmem_limit_bytes=limit * 1024 * 1024),
        cost_estimate=cost(flops, 16 * 1024 * 1024),
    )(*args)


def expert_own(core, own, gate_w, up_w, down_w):
    rows, double = own.shape
    units = gate_w.shape[1]
    width = double // 2
    shapes = [((rows, units), F32)] * 3 + [((width, units), BF16)] * 4 + [((units, width), BF16)]
    return pl.pallas_call(
        own_body,
        in_specs=[IN_SMEM] + [IN_HBM] * 4,
        out_specs=[IN_VMEM] * len(shapes),
        out_shape=[jax.ShapeDtypeStruct(s, d) for s, d in shapes],
        scratch_shapes=[
            pltpu.VMEM((2, rows // 2, double), BF16),
            pltpu.VMEM((units, width), BF16),
            pltpu.SemaphoreType.DMA((8,)),
        ],
        compiler_params=pltpu.CompilerParams(vmem_limit_bytes=12 * 1024 * 1024),
        name="expert_own",
        cost_estimate=cost(3 * rows * double * units, 10 * double * units),
    )(core, *[in_hbm(array) for array in (own, gate_w, up_w, down_w)])


def expert_peer(start, peer, gate_w, up_w, down_w, *parts):
    rows, double = peer.shape[0] // 2, peer.shape[1]
    units = gate_w.shape[1]
    outs = [((rows, units), BF16)] * 2 + [((rows, double // 2), BF16)]

    def body(*refs):
        peer_body(start, *refs)

    return pl.pallas_call(
        body,
        in_specs=[IN_HBM] + [IN_VMEM] * 6,
        out_specs=[IN_HBM] + [IN_VMEM] * len(outs),
        out_shape=[pltpu.HBM((rows, units), BF16)] + [jax.ShapeDtypeStruct(s, d) for s, d in outs],
        scratch_shapes=[
            pltpu.VMEM((rows, double), BF16),
            pltpu.VMEM((rows, units), BF16),
            pltpu.SemaphoreType.DMA((3,)),
        ],
        compiler_params=pltpu.CompilerParams(vmem_limit_bytes=16 * 1024 * 1024),
        name="expert_peer",
        cost_estimate=cost(5 * rows * double * units, 8 * rows * double),
    )(in_hbm(peer), gate_w, up_w, down_w, *parts)


def expert_mine(gate_a, gate_b, up_a, up_b, gate_w, up_w):
    rows, width = 2 * gate_a.shape[0], gate_w.shape[0]
    flops = 4 * rows * width * gate_w.shape[1]
    outs = [((rows, width), BF16)]
    return on_chip(mine_body, outs, flops, 8, gate_a, gate_b, up_a, up_b, gate_w, up_w)[0]


def add_parts(mine, other_a, other_b):
    rows, width = mine.shape
    blocks = 4
    return pl.pallas_call(
        add_body,
        in_specs=[IN_VMEM] * 3,
        out_specs=pl.BlockSpec(memory_space=pltpu.HBM),
        out_shape=pltpu.HBM(mine.shape, BF16),
        scratch_shapes=[
            pltpu.VMEM((blocks, rows // blocks, width), BF16),
            pltpu.SemaphoreType.DMA((blocks,)),
        ],
        compiler_params=pltpu.CompilerParams(vmem_limit_bytes=8 * 1024 * 1024),
        name="add_parts",
        cost_estimate=cost(mine.size, 6 * mine.size),
    )(mine, other_a, other_b)


def tick_body(in_ref, out_ref):
    out_ref[...] = in_ref[...]


def tick(array):
    return pl.pallas_call(
        tick_body, out_shape=jax.ShapeDtypeStruct(array.shape, array.dtype), name="carry"
    )(array)


def product_body(left_ref, right_ref, out_ref):
    out_ref[...] = dot_tn(left_ref[...], right_ref[...])


def product_more_body(left_ref, right_ref, part_ref, out_ref):
    out_ref[...] = (part_ref[...] + dot_tn(left_ref[...], right_ref[...])).astype(BF16)


def product(left, right, *part):
    body = product_more_body if part else product_body
    outs = [((left.shape[1], right.shape[1]), BF16 if part else F32)]
    flops = 2 * left.size * right.shape[1]
    return on_chip(body, outs, flops, 8, left, right, *part)[0]


def conv_body(
    delta_ref, rim_ref, taps_ref, gate_ref, input_ref, input_grad_ref, gate_grad_ref
):
    delta = delta_ref[...]
    rows = delta.shape[0]
    row = lax.broadcasted_iota(jnp.int32, delta.shape, 0)
    first, second = rim_ref[0:1, :], rim_ref[1:2, :]
    next_one = jnp.where(row == rows - 1, first, pltpu.roll(delta, rows - 1, 0))
    next_two = jnp.where(row == rows - 2, first, pltpu.roll(delta, rows - 2, 0))
    next_two = jnp.where(row == rows - 1, second, next_two)
    grad = taps_ref[2:3, :] * delta + taps_ref[1:2, :] * next_one + taps_ref[0:1, :] * next_two
    input_grad_ref[...] = (grad * gate_ref[...].astype(F32)).astype(BF16)
    gate_grad_ref[...] = (grad * input_ref[...].astype(F32)).astype(BF16)


def conv_back(delta, rim, taps, gate, inputs):
    return pl.pallas_call(
        conv_body,
        in_specs=[IN_VMEM] * 5,
        out_specs=[IN_VMEM] * 2,
        out_shape=[jax.ShapeDtypeStruct(delta.shape, BF16)] * 2,
        compiler_params=pltpu.CompilerParams(vmem_limit_bytes=12 * 1024 * 1024),
        name="conv_back",
        cost_estimate=cost(12 * delta.size, 12 * delta.size),
    )(delta, rim, taps, gate, inputs)


def mixer_body(
    core_ref, grad_hbm, peer_hbm, proj_hbm, gate_ref, conv_ref, delta_ref, out_ref,
    grad_ref, peer_ref, proj_ref, sems,
):
    width = grad_ref.shape[1]
    mine = pl.multiple_of(core_ref[0] * width, width)
    other = pl.multiple_of((1 - core_ref[0]) * width, width)
    moves = (
        (proj_hbm.at[pl.ds(mine, width), :], proj_ref.at[0]),
        (grad_hbm, grad_ref),
        (proj_hbm.at[pl.ds(other, width), :], proj_ref.at[1]),
        (peer_hbm, peer_ref),
    )
    copies = [pltpu.make_async_copy(a, b, sems.at[i]) for i, (a, b) in enumerate(moves)]
    for copy in copies:
        copy.start()
    copies[0].wait()
    copies[1].wait()
    mixer_grad = dot_nn(grad_ref[...], proj_ref[0])
    copies[2].wait()
    copies[3].wait()
    mixer_grad = mixer_grad + dot_nn(peer_ref[...], proj_ref[1])
    delta_ref[...] = mixer_grad * gate_ref[...].astype(F32)
    out_ref[...] = (mixer_grad * conv_ref[...]).astype(BF16)


def mixer_back(core, grad, peer, proj, gate, conv):
    rows, width = grad.shape
    channels = proj.shape[1]
    return pl.pallas_call(
        mixer_body,
        in_specs=[IN_SMEM] + [IN_HBM] * 3 + [IN_VMEM] * 2,
        out_specs=[IN_VMEM] * 2,
        out_shape=[
            jax.ShapeDtypeStruct((rows, channels), F32),
            jax.ShapeDtypeStruct((rows, channels), BF16),
        ],
        scratch_shapes=[
            pltpu.VMEM((rows, width), BF16),
            pltpu.VMEM((rows, width), BF16),
            pltpu.VMEM((2, width, channels), BF16),
            pltpu.SemaphoreType.DMA((4,)),
        ],
        compiler_params=pltpu.CompilerParams(vmem_limit_bytes=12 * 1024 * 1024),
        name="mixer_back",
        cost_estimate=cost(4 * rows * width * channels, 8 * 1024 * 1024),
    )(core, in_hbm(grad), in_hbm(peer), in_hbm(proj), gate, conv)


def weights_body(
    core_ref, own_x, own_y, peer_x, peer_y, hidden_a, hidden_b, gate_a, gate_b, up_a, up_b,
    gate_out, up_out, down_out,
):
    half = hidden_a.shape[0]

    def emit(x_ref, y_ref):
        x_a, x_b = x_ref[:half, :], x_ref[half:, :]
        gate_out[...] = dot_tn(x_a, gate_a[...]) + dot_tn(x_b, gate_b[...])
        up_out[...] = dot_tn(x_a, up_a[...]) + dot_tn(x_b, up_b[...])
        down_out[...] = dot_tn(hidden_a[...], y_ref[:half, :]) + dot_tn(
            hidden_b[...], y_ref[half:, :]
        )

    steps = pl.num_programs(0) // 2

    @pl.when(pl.program_id(0) < steps)
    def _():
        emit(own_x, own_y)

    @pl.when(pl.program_id(0) >= steps)
    def _():
        emit(peer_x, peer_y)


def weight_grads(core, own, peer, *halves):
    rows, double = own.shape
    width = double // 2
    units = halves[0].shape[1]
    chunk = 256
    half = width // chunk

    def own_at(base):
        return pl.BlockSpec((rows, chunk), lambda s, c: (0, base + jnp.minimum(s, half - 1)))

    def peer_at(base):
        return pl.BlockSpec((rows, chunk), lambda s, c: (0, base + jnp.maximum(s - half, 0)))

    def place(s, c):
        side = jnp.where(s < half, c[0], 1 - c[0])
        return side * half + jnp.where(s < half, s, s - half)

    whole = pl.BlockSpec((rows // 2, units), lambda s, c: (0, 0))
    tall = pl.BlockSpec((chunk, units), lambda s, c: (place(s, c), 0))
    wide = pl.BlockSpec((units, chunk), lambda s, c: (0, place(s, c)))
    return pl.pallas_call(
        weights_body,
        grid_spec=pltpu.PrefetchScalarGridSpec(
            num_scalar_prefetch=1,
            grid=(2 * half,),
            in_specs=[own_at(0), own_at(half), peer_at(0), peer_at(half)] + [whole] * 6,
            out_specs=[tall, tall, wide],
        ),
        out_shape=[
            jax.ShapeDtypeStruct((double, units), F32),
            jax.ShapeDtypeStruct((double, units), F32),
            jax.ShapeDtypeStruct((units, double), F32),
        ],
        compiler_params=pltpu.CompilerParams(vmem_limit_bytes=VMEM),
        name="weight_grads",
        cost_estimate=cost(12 * rows * width * units, 24 * width * units),
    )(core, own, own, peer, peer, *halves)


def stage(
    stream,
    norm_gain,
    cotangent,
    route_weights,
    routes,
    conv_input,
    conv_bgate,
    conv_cgate,
    conv_taps,
    out_proj,
    gate_weight,
    up_weight,
    down_weight,
):
    experts = lax.axis_size(SP)
    tok_count, width = stream.shape
    top_count = routes.shape[1]
    capacity = 2 * tok_count * top_count // experts
    slots = experts * capacity
    core = lax.axis_index("tp")
    core_arg = core.astype(jnp.int32).reshape(1)
    gain_row = norm_gain[None, :]

    squares, target = find_slots(stream, routes.T, experts, capacity)
    peer_squares = swap(squares)
    rows, selector, inverse_row = build_rows(
        target, route_weights.T, squares, peer_squares, stream, cotangent, gain_row, slots
    )
    own = exchange(rows.reshape(experts, capacity, 2 * width), SP)
    own = own.reshape(slots, 2 * width)

    input_float = conv_input.astype(F32)
    cgate_float = conv_cgate.astype(F32)
    bgate_float = conv_bgate.astype(F32)
    rim_rows = shifted(jnp.stack([conv_input[-2:], conv_cgate[-2:]]), SP, 1)
    rim_gated = rim_rows[1].astype(F32) * rim_rows[0].astype(F32)
    gated = cgate_float * input_float
    extended = jnp.concatenate([rim_gated, gated], axis=0)
    conv_out = (
        conv_taps[0][None, :] * extended[:-2]
        + conv_taps[1][None, :] * extended[1:-1]
        + conv_taps[2][None, :] * extended[2:]
    )
    mixer_out = (bgate_float * conv_out).astype(BF16)
    line = lax.axis_size("sp_0")
    spot = lax.axis_index("sp_0")
    token_half = tok_count // 2
    channels = mixer_out.shape[1]

    def half_of(array, which, dim):
        return lax.dynamic_slice_in_dim(array, which * token_half, token_half, dim)

    inverse_row = tick(inverse_row)
    peer = swap(own)
    around = [mixer_out]
    for step in range(1, line):
        around.append(turned(mixer_out, "sp_0", step))
    gate_part, up_part, grad_part, gate_own, up_own, gate_peer, up_peer, down_peer = expert_own(
        core_arg, own, gate_weight[0], up_weight[0], down_weight[0]
    )
    more = (gate_peer, up_peer, down_peer, gate_part, up_part, grad_part)
    hidden_a, gate_a, up_a, theirs_a = expert_peer(0, peer, *more)
    other_a = swap(theirs_a)
    hidden_b, gate_b, up_b, theirs_b = expert_peer(slots // 2, peer, *more)
    other_b = swap(theirs_b)
    part_mine = expert_mine(gate_a, gate_b, up_a, up_b, gate_own, up_own)
    row_grads = add_parts(part_mine, other_a, other_b)
    returned = exchange(row_grads.reshape(experts, capacity, width), SP).reshape(slots, width)
    halves = (hidden_a, hidden_b, gate_a, gate_b, up_a, up_b)
    grads_w = weight_grads(core_arg, own, peer, *halves)
    around = jnp.stack(around)
    mixers = jnp.concatenate(
        [lax.dynamic_slice_in_dim(around, (spot - k) % line, 1, 0) for k in range(line)], axis=0
    )
    mixers_mine = half_of(mixers, core, 1).reshape(line * token_half, channels)
    mixers_theirs = half_of(mixers, 1 - core, 1).reshape(line * token_half, channels)
    returned, (gate_g, up_g, down_g), mixers_mine, mixers_theirs = lax.optimization_barrier(
        (returned, grads_w, mixers_mine, mixers_theirs)
    )

    normed_grad = dot_tn(selector, returned)
    stream_float = stream.astype(F32)
    cot_float = cotangent.astype(F32)
    inverse = inverse_row[0][:, None]
    cross_part = jnp.sum(stream_float * gain_row * normed_grad, axis=1)
    cross = cross_part + swap(cross_part)
    stream_grad = (
        cot_float
        + inverse * gain_row * normed_grad
        - stream_float * inverse * inverse * inverse * cross[:, None] / D
    ).astype(BF16)

    grad_peer = swap(stream_grad)
    mine_half, peer_half = half_of(stream_grad, core, 0), half_of(grad_peer, core, 0)
    low = jnp.where(core == 0, mine_half, peer_half)
    high = jnp.where(core == 0, peer_half, mine_half)
    quarter = 2 * width // line
    parts = [low[:, :quarter], low[:, quarter:], high[:, :quarter], high[:, quarter:]]
    sent = jnp.stack(parts)
    grads_mine = exchange(sent, "sp_0").reshape(line * token_half, quarter)
    delta, bgate_grad = mixer_back(core_arg, stream_grad, grad_peer, out_proj, conv_bgate, conv_out)
    next_rim = shifted(delta[:2], SP, -1)
    late_taps = tick(conv_taps)
    grads_theirs = swap(grads_mine)
    proj_part = product(grads_theirs, mixers_theirs, product(grads_mine, mixers_mine))
    plane = lax.axis_size(("sp_1", "sp_2"))
    arrived = exchange(proj_part.reshape(plane, quarter // plane, channels), ("sp_1", "sp_2"))
    proj_grad = arrived.astype(F32).sum(axis=0)

    input_grad, cgate_grad = conv_back(delta, next_rim, late_taps, conv_cgate, conv_input)
    return (
        stream_grad,
        proj_grad,
        input_grad,
        bgate_grad,
        cgate_grad,
        gate_g[None],
        up_g[None],
        down_g[None],
    )


def solution(mesh):
    finer = Mesh(mesh.devices.reshape(4, 4, 4, mesh.shape["tp"]), ("sp_0", "sp_1", "sp_2", "tp"))
    return jax.shard_map(
        stage,
        mesh=finer,
        in_specs=(
            P(SP, "tp"),
            P("tp"),
            P(SP, "tp"),
            P(SP, None),
            P(SP, None),
            P(SP, "tp"),
            P(SP, "tp"),
            P(SP, "tp"),
            P(None, "tp"),
            P(None, "tp"),
            P(SP, None, "tp"),
            P(SP, None, "tp"),
            P(SP, "tp", None),
        ),
        out_specs=(
            P(SP, "tp"),
            P(SP, "tp"),
            P(SP, "tp"),
            P(SP, "tp"),
            P(SP, "tp"),
            P(SP, None, "tp"),
            P(SP, None, "tp"),
            P(SP, "tp", None),
        ),
        check_vma=False,
    )
```
